32 devices in a mesh: sp: 8 (over z, x), tp: 4 (over y, core).
Axes of the slice: x: 2, y: 2, z: 4, core: 2. Of those that a mesh axis runs over, the one named last changes fastest.
Arguments:
- query_narrow: bfloat16 [2048, 1024], P('sp', 'tp'), may hold values from -6 to 6
- key_narrow: bfloat16 [2048, 1024], P('sp', 'tp'), may hold values from -6 to 6
- value_narrow: bfloat16 [2048, 1024], P('sp', 'tp'), may hold values from -12 to 12
- query_broad: bfloat16 [2048, 1024], P('sp', 'tp'), may hold values from -6 to 6
- key_broad: bfloat16 [2048, 1024], P('sp', 'tp'), may hold values from -6 to 6
- value_broad: bfloat16 [2048, 1024], P('sp', 'tp'), may hold values from -12 to 12
- offset_narrow: bfloat16 [16, 2048], P('tp', 'sp'), as said below
- offset_broad: bfloat16 [8, 2048], P('tp', 'sp'), as said below
- residual: bfloat16 [2048, 2048], P(('sp', 'tp')), may hold values from -6 to 6
- out_narrow: bfloat16 [1024, 2048], P('tp'), may hold values from -0.25 to 0.25
- out_broad: bfloat16 [1024, 2048], P('tp'), may hold values from -0.25 to 0.25
- norm_gain: float32 [2048], replicated, may hold values from 0.1 to 1.9
- up_proj: bfloat16 [2048, 8192], P('sp', 'tp'), may hold values from -0.125 to 0.125
- down_proj: bfloat16 [8192, 2048], P('tp', 'sp'), may hold values from -0.0625 to 0.0625
Outputs:
- output: bfloat16 [2048, 2048], P(('sp', 'tp'))
The draws below stay inside these ranges and needn't reach their ends.
Inputs may be any that keep to these rules, and one draw needn't show every extreme that they name: `offset_narrow`: additive score offsets of each head for each key position. `offset_broad`: additive score offsets of each head for each key position.
All inputs are finite; a program needn't handle non-finite values.
Results may differ from the reference program's by a relative error of at most 0.018.
Values may be sent and summed in bfloat16 or wider, within the bound.
A program may use at most 64 MiB of HBM per device.

```python
import math
import jax
import jax.numpy as jnp
from jax import lax

D = 2048
FF = 8192
NARROW_HEADS = 16
NARROW_SIZE = 64
BROAD_HEADS = 8
BROAD_SIZE = 128
TOKENS_PER_SHARD = 256
SEQUENCE_TOKENS = 2048


def stick_offsets(key, total_heads, salt):
    key = jax.random.fold_in(key, salt)
    random_subkeys = jax.random.split(key, 6)
    gradual_drift = jax.random.randint(random_subkeys[0], (total_heads, 1), 0, 2).astype(jnp.float32)
    slow_base = -jnp.log(jnp.float32(SEQUENCE_TOKENS)) - 2.0
    fast_base = -jnp.log(jnp.float32(40.0)) - 0.5
    base_value = gradual_drift * slow_base + (1.0 - gradual_drift) * fast_base
    base_value = base_value + jax.random.uniform(random_subkeys[1], (total_heads, 1), jnp.float32, -0.3, 0.3)
    slope_factor = jax.random.uniform(random_subkeys[2], (total_heads, SEQUENCE_TOKENS // TOKENS_PER_SHARD), jnp.float32, -0.7, 0.7)
    slope_factor = jnp.repeat(slope_factor, TOKENS_PER_SHARD, axis=1)
    jagged_noise = 0.5 * jax.random.truncated_normal(random_subkeys[3], -2.0, 2.0, (total_heads, SEQUENCE_TOKENS), jnp.float32)
    spike_amount = (jax.random.randint(random_subkeys[4], (total_heads, SEQUENCE_TOKENS), 0, 2 * TOKENS_PER_SHARD) == 0).astype(jnp.float32) * gradual_drift
    spike_height = jax.random.uniform(random_subkeys[5], (total_heads, SEQUENCE_TOKENS), jnp.float32, -1.9, -0.9)
    shift_amount = spike_amount * spike_height + (1.0 - spike_amount) * (base_value + slope_factor + jagged_noise)
    return shift_amount.astype(jnp.bfloat16)


def draw_offset_narrow(key, part):
    return stick_offsets(key, NARROW_HEADS, 11)


def draw_offset_broad(key, part):
    return stick_offsets(key, BROAD_HEADS, 23)


def level_of(own_key, shape, cuts, low, top_value):
    factor_of, own = 1.0, jax.random.fold_in(own_key, 6)
    for dim, parts in cuts:
        draws = jnp.exp(jax.random.uniform(jax.random.fold_in(own, dim), (parts,), jnp.float32, low / len(cuts), top_value / len(cuts)))
        factor_of = factor_of * jnp.repeat(draws, shape[dim] // parts).reshape([-1 if axis == dim else 1 for axis in range(len(shape))])
    return factor_of


def centred(stream_key, extent, spread, bound, pieces=(), held_as=jnp.bfloat16):
    result = spread * jax.random.normal(stream_key, extent, jnp.float32)
    if pieces:
        result = result * level_of(stream_key, extent, pieces, -0.22, 0.18)
    return jnp.clip(result, -bound, bound).astype(held_as)


def setup_inputs(seed: int = 0) -> dict:
    arg_keys = jax.random.split(jax.random.key(seed), 15)
    query_narrow = centred(arg_keys[0], (SEQUENCE_TOKENS, NARROW_HEADS * NARROW_SIZE), 1.0, 6.0, ((0, 8), (1, 4)))
    key_narrow = centred(arg_keys[1], (SEQUENCE_TOKENS, NARROW_HEADS * NARROW_SIZE), 1.0, 6.0, ((0, 8), (1, 4)))
    value_narrow = centred(arg_keys[2], (SEQUENCE_TOKENS, NARROW_HEADS * NARROW_SIZE), 2.0, 12.0, ((0, 8), (1, 4)))
    query_broad = centred(arg_keys[3], (SEQUENCE_TOKENS, BROAD_HEADS * BROAD_SIZE), 1.0, 6.0, ((0, 8), (1, 4)))
    key_broad = centred(arg_keys[4], (SEQUENCE_TOKENS, BROAD_HEADS * BROAD_SIZE), 1.0, 6.0, ((0, 8), (1, 4)))
    value_broad = centred(arg_keys[5], (SEQUENCE_TOKENS, BROAD_HEADS * BROAD_SIZE), 2.0, 12.0, ((0, 8), (1, 4)))
    offset_narrow = draw_offset_narrow(jax.random.fold_in(arg_keys[14], 71), 0)
    offset_broad = draw_offset_broad(jax.random.fold_in(arg_keys[14], 71), 0)
    residual = centred(arg_keys[8], (SEQUENCE_TOKENS, D), 1.0, 6.0, ((0, 32),))
    out_narrow = centred(arg_keys[9], (NARROW_HEADS * NARROW_SIZE, D), ((NARROW_HEADS * NARROW_SIZE + BROAD_HEADS * BROAD_SIZE) // 4) ** -0.5, 0.25, ((0, 4),))
    out_broad = centred(arg_keys[10], (BROAD_HEADS * BROAD_SIZE, D), ((NARROW_HEADS * NARROW_SIZE + BROAD_HEADS * BROAD_SIZE) // 4) ** -0.5, 0.25, ((0, 4),))
    norm_gain = jnp.clip(1.0 + 0.18 * jax.random.normal(arg_keys[11], (D,), jnp.float32), 0.1, 1.9)
    up_proj = centred(arg_keys[12], (D, FF), D ** -0.5, 0.125, ((0, 8), (1, 4)))
    down_proj = centred(arg_keys[13], (FF, D), FF ** -0.5, 0.0625, ((0, 4), (1, 8)))
    return {"query_narrow": query_narrow, "key_narrow": key_narrow, "value_narrow": value_narrow, "query_broad": query_broad, "key_broad": key_broad, "value_broad": value_broad, "offset_narrow": offset_narrow, "offset_broad": offset_broad, "residual": residual, "out_narrow": out_narrow, "out_broad": out_broad, "norm_gain": norm_gain, "up_proj": up_proj, "down_proj": down_proj}


def stick_group(query, key, value, shift_amount, total_heads, head_size):
    tokens = query.shape[0]
    span_rows = math.gcd(tokens, 512)
    blocks = tokens // span_rows
    q_all = query.astype(jnp.float32).reshape(tokens, total_heads, head_size)
    k_all = key.astype(jnp.float32).reshape(tokens, total_heads, head_size)
    v_all = value.astype(jnp.float32).reshape(tokens, total_heads, head_size)
    off_all = shift_amount.astype(jnp.float32)

    def query_block(index):
        q_start = index * span_rows
        q_block = lax.dynamic_slice_in_dim(q_all, q_start, span_rows, 0)
        query_pos = q_start + jnp.arange(span_rows, dtype=jnp.int32)

        def key_block(turn_index, state):
            keep_sum, running = state
            k_start = (index - turn_index) * span_rows
            k_block = lax.dynamic_slice_in_dim(k_all, k_start, span_rows, 0)
            v_block = lax.dynamic_slice_in_dim(v_all, k_start, span_rows, 0)
            o_block = lax.dynamic_slice_in_dim(off_all, k_start, span_rows, 1)
            key_pos = k_start + jnp.arange(span_rows, dtype=jnp.int32)
            scores = jnp.einsum('qhe,khe->hqk', q_block, k_block) * head_size ** (-0.5) + o_block[:, None, :]
            causal = (key_pos[None, :] < query_pos[:, None])[None]
            log_keep = jnp.where(causal, jax.nn.log_sigmoid(-scores), jnp.float32(0.0))
            keep_after = lax.cumsum(log_keep, axis=2, reverse=True) - log_keep
            weight = jnp.where(causal, jnp.exp(jax.nn.log_sigmoid(scores) + keep_after + keep_sum[:, :, None]), jnp.float32(0.0))
            rounded = lax.optimization_barrier(weight.astype(jnp.bfloat16)).astype(jnp.float32)
            running = running + jnp.einsum('hqk,khe->qhe', rounded, v_block)
            return (keep_sum + lax.optimization_barrier(jnp.sum(log_keep, axis=2)), running)
        start_state = (jnp.zeros((total_heads, span_rows), jnp.float32), jnp.zeros((span_rows, total_heads, head_size), jnp.float32))
        keep_sum, running = lax.fori_loop(jnp.int32(0), index + 1, key_block, start_state)
        return running.reshape(span_rows, total_heads * head_size)
    mixed = lax.map(query_block, jnp.arange(blocks, dtype=jnp.int32))
    return mixed.reshape(tokens, total_heads * head_size).astype(jnp.bfloat16)

def reference(query_narrow, key_narrow, value_narrow, query_broad, key_broad, value_broad, offset_narrow, offset_broad, residual, out_narrow, out_broad, norm_gain, up_proj, down_proj):
    mixed_narrow = stick_group(query_narrow, key_narrow, value_narrow, offset_narrow, NARROW_HEADS, NARROW_SIZE)
    mixed_broad = stick_group(query_broad, key_broad, value_broad, offset_broad, BROAD_HEADS, BROAD_SIZE)
    attended = jnp.dot(mixed_narrow, out_narrow, preferred_element_type=jnp.float32) + jnp.dot(mixed_broad, out_broad, preferred_element_type=jnp.float32)
    updated = residual.astype(jnp.float32) + attended
    scale = lax.rsqrt(lax.optimization_barrier(jnp.mean(updated * updated, axis=-1, keepdims=True)) + 1e-06)
    normed = (updated * scale * norm_gain).astype(jnp.bfloat16)
    hidden = jnp.square(jax.nn.relu(jnp.dot(normed, up_proj, preferred_element_type=jnp.float32))).astype(jnp.bfloat16)
    return (updated + jnp.dot(hidden, down_proj, preferred_element_type=jnp.float32)).astype(jnp.bfloat16)
```

```python
import functools

import jax
import jax.numpy as jnp
from jax import lax
from jax.experimental import pallas as pl
from jax.experimental.pallas import tpu as pltpu
from jax.sharding import PartitionSpec as P

NARROW_SIZE = 64
BROAD_SIZE = 128
F32 = jnp.float32
BF16 = jnp.bfloat16


def ring_order(shards):
    across = 1 << ((shards.bit_length() - 1) // 2)
    along = shards // across
    order = [z * across for z in range(along)]
    for turn, z in enumerate(reversed(range(along))):
        row = list(range(1, across))
        if turn % 2:
            row.reverse()
        order += [z * across + x for x in row]
    return order


def lookup(table, index):
    found = jnp.int32(0)
    for place, value in enumerate(table):
        found = found + jnp.where(index == place, jnp.int32(value), jnp.int32(0))
    return found


def kernel(
    shards, peers, order, across, cores,
    q_n, q_b, k_n, v_n, k_b, v_b, off_n, off_b, residual, out_n, out_b, gain, up, down,
    o_ref,
    kv_slots, off_slots, up_src, down_src, up_buf, down_buf, mixed, part, inbox, updated,
    normed_all, hidden, channel, half_out, half_in, rows_out, rows_in,
    kv_send, kv_recv, a_send, a_recv, x_send, y_send, b_recv, tp_send, tp_recv,
    n_send, n_recv, h_send, h_recv, r_send, r_recv, load_sems,
):
    tok = q_n.shape[0]
    model = part.shape[1]
    rows = residual.shape[0]
    depth, wide = up.shape
    along, lanes = shards // across, peers // cores
    group = along * cores
    unit = wide // group
    me = lax.axis_index("sp")
    me_tp = lax.axis_index("tp")
    z, x = lax.div(me, across), lax.rem(me, across)
    y, c = lax.div(me_tp, cores), lax.rem(me_tp, cores)

    def turn(value, by, size):
        return lax.rem(value + by, size)

    def place(dz=0, dx=0, dy=0, dc=0):
        return (
            turn(z, dz, along) * across + turn(x, dx, across),
            turn(y, dy, lanes) * cores + turn(c, dc, cores),
        )

    def remote(src, dst, send_sem, recv_sem, where):
        return pltpu.make_async_remote_copy(
            src_ref=src, dst_ref=dst, send_sem=send_sem, recv_sem=recv_sem,
            device_id=where, device_id_type=pl.DeviceIdType.MESH,
        )

    started = []

    def launch(copy):
        copy.start()
        started.append(copy)

    inverse = [order.index(s) for s in range(shards)]
    pos = lookup(inverse, me)
    right = lookup(order, lax.rem(pos + 1, shards))
    left = lookup(order, lax.rem(pos + shards - 1, shards))

    def piece(m, shard, column):
        if m == 0:
            return up_buf.at[column, pl.ds(pl.multiple_of(shard * depth, depth), depth)]
        return down_buf.at[shard, pl.ds(pl.multiple_of(column * unit, unit), unit)]

    def block(m, shard, lane):
        if m == 0:
            return up_buf.at[
                pl.ds(lane * cores, cores), pl.ds(pl.multiple_of(shard * depth, depth), depth)
            ]
        size = cores * unit
        return down_buf.at[shard, pl.ds(pl.multiple_of(lane * size, size), size)]

    loads = []
    for way, (k, v, off) in enumerate(((k_n, v_n, off_n), (k_b, v_b, off_b))):
        loads += [
            (k, kv_slots.at[way, 0, pl.ds(0, tok)]),
            (v, kv_slots.at[way, 0, pl.ds(tok, tok)]),
            (off, off_slots.at[way, 0]),
        ]
    mine = pl.ds(pl.multiple_of((z * cores + c) * unit, unit), unit)
    weight_loads = [
        (up.at[:, pl.ds(j * unit, unit)], up_src.at[j]) for j in range(group)
    ] + [
        (down, down_src),
        (up.at[:, mine], piece(0, me, me_tp)),
        (down.at[mine], piece(1, me, me_tp)),
    ]
    loads = [
        pltpu.make_async_copy(src, dst, load_sems.at[i])
        for i, (src, dst) in enumerate(loads + weight_loads)
    ]
    for load in loads:
        load.start()
    weight_loads = loads[6:]
    loads = loads[:6]

    barrier = pltpu.get_barrier_semaphore()
    friends = [
        place(dz=dz, dc=dc) for dz in range(along) for dc in range(cores) if dz or dc
    ]
    friends += [place(dx=dx) for dx in range(1, across)]
    friends += [place(dy=dy, dc=dc) for dy in range(1, lanes) for dc in range(cores)]
    for friend in friends:
        pl.semaphore_signal(
            barrier, inc=1, device_id=friend, device_id_type=pl.DeviceIdType.MESH
        )
    pl.semaphore_wait(barrier, len(friends))

    def stream(kind, way, t):
        if kind == 0:
            return off_slots.at[way, t]
        return kv_slots.at[way, t, pl.ds((kind - 1) * tok, tok)]

    def hop(kind, way, t):
        return remote(
            stream(kind, way, t), stream(kind, way, t + 1),
            kv_send.at[way, kind, t], kv_recv.at[way, kind, t],
            ((left if way else right), me_tp),
        )

    def each(first, last, body):
        def step(t, carry):
            body(t)
            return carry

        lax.fori_loop(first, last, step, 0)

    def relay(t):
        for kind in range(3):
            for way in range(2):
                hop(kind, way, t - 1).wait_recv()
                hop(kind, way, t).start()

    def exchange(m, dz, dc):
        to = turn(z, dz, along) * cores + turn(c, dc, cores)
        if m == 0:
            src = up_src.at[to]
        else:
            src = down_src.at[pl.ds(pl.multiple_of(to * unit, unit), unit)]
        return remote(
            src, piece(m, me, me_tp), a_send.at[m, dz, dc], a_recv.at[m, dz, dc],
            place(dz=dz, dc=dc),
        )

    def send_column(m):
        for dz in range(along):
            for dc in range(cores):
                if dz or dc:
                    launch(exchange(m, dz, dc))

    def origin(dz, bx=0):
        return turn(z, along - dz, along) * across + turn(x, bx, across)

    def along_x(m, dz, by, dx):
        held = block(m, origin(dz), turn(y, by, lanes))
        return remote(
            held, held, x_send.at[m, dz, by, dx], b_recv.at[m, dz, (across - dx) % across, by],
            place(dx=dx),
        )

    def along_y(m, dz, bx, dy):
        held = block(m, origin(dz, bx), y)
        return remote(
            held, held, y_send.at[m, dz, bx, dy], b_recv.at[m, dz, bx, (lanes - dy) % lanes],
            place(dy=dy),
        )

    def await_block(m, dz, bx, by):
        held = block(m, origin(dz, bx), turn(y, by, lanes))
        remote(
            held, held, x_send.at[m, dz, 0, 0], b_recv.at[m, dz, bx, by], place(dc=1)
        ).wait_recv()

    def spread_block(m, dz):
        for dc in range(cores):
            if dz or dc:
                exchange(m, dz, dc).wait_recv()
        for dx in range(1, across):
            launch(along_x(m, dz, 0, dx))
        for dy in range(1, lanes):
            launch(along_y(m, dz, 0, dy))

    def relay_block(m, dz):
        if dz % 2 == 0:
            for bx in range(1, across):
                await_block(m, dz, bx, 0)
                for dy in range(1, lanes):
                    launch(along_y(m, dz, bx, dy))
        else:
            for by in range(1, lanes):
                await_block(m, dz, 0, by)
                for dx in range(1, across):
                    launch(along_x(m, dz, by, dx))

    def finish_weights(m):
        for dz in range(along):
            for bx in range(across):
                for by in range(lanes):
                    if bx and by or (by if dz % 2 == 0 else bx):
                        await_block(m, dz, bx, by)

    for load in loads:
        load.wait()
    for kind in range(3):
        for way in range(2):
            hop(kind, way, 0).start()
    for load in weight_loads:
        load.wait()
    each(1, shards - 1, relay)
    for kind in range(3):
        for way in range(2):
            hop(kind, way, shards - 2).wait_recv()

    send_column(0)
    send_column(1)
    spread_block(0, 0)
    spread_block(1, 0)

    row_at = lax.broadcasted_iota(jnp.int32, (tok, tok), 0)
    col_at = lax.broadcasted_iota(jnp.int32, (tok, tok), 1)
    later = (row_at > col_at).astype(BF16)
    later2 = jnp.concatenate([later, later], axis=0)
    heads = []
    for way, (q, size) in enumerate(((q_n, NARROW_SIZE), (q_b, BROAD_SIZE))):
        for h in range(q.shape[1] // size):
            heads.append((way, h, size, q))

    def head_block(way, h, size, q, at, keep_sum, diagonal):
        there = lookup(inverse, at)
        slot = lax.rem((there - pos if way else pos - there) + shards, shards)
        cols = pl.ds(h * size, size)
        keys = kv_slots[way, slot, pl.ds(0, tok), cols]
        values = kv_slots[way, slot, pl.ds(tok, tok), cols]
        offset = off_slots[way, slot].astype(F32)[h : h + 1, :]
        scores = lax.dot_general(
            q[:, cols], keys, (((1,), (1,)), ((), ())), preferred_element_type=F32
        ) * (size ** -0.5) + offset
        keep = -(jnp.maximum(scores, 0.0) + jnp.log(1.0 + jnp.exp(-jnp.abs(scores))))
        breaks = scores + keep
        if diagonal:
            keep = jnp.where(col_at < row_at, keep, 0.0)
        high = keep.astype(BF16)
        low = (keep - high.astype(F32)).astype(BF16)
        after = jnp.dot(
            jnp.concatenate([high, low], axis=1), later2, preferred_element_type=F32
        )
        weight = jnp.exp(breaks + after + keep_sum)
        if diagonal:
            weight = jnp.where(col_at < row_at, weight, 0.0)
        added = jnp.dot(weight.astype(BF16), values, preferred_element_type=F32)
        return keep_sum + (after[:, :1] + keep[:, :1]), added

    chores = []
    for dz in range(1, along):
        chores.append(functools.partial(spread_block, 0, dz))
        chores.append(functools.partial(relay_block, 0, dz - 1))
    for index, (way, h, size, q) in enumerate(heads):
        start = head_block(way, h, size, q, me, jnp.zeros((tok, 1), F32), True)

        def sweep(at, state, way=way, h=h, size=size, q=q):
            keep_sum, running = state
            keep_sum, added = head_block(way, h, size, q, me - 1 - at, keep_sum, False)
            return keep_sum, running + added

        _, running = lax.fori_loop(0, me, sweep, start)
        base = way * q_n.shape[1] + h * size
        mixed[:, pl.ds(base, size)] = running.astype(BF16)
        share = len(chores) * (index + 1) // len(heads) - len(chores) * index // len(heads)
        first_chore = len(chores) * index // len(heads)
        for chore in chores[first_chore : first_chore + share]:
            chore()

    tile = min(512, model)
    n_cols = out_n.shape[0]

    def project(i):
        cols = pl.ds(pl.multiple_of(i * tile, tile), tile)
        part[:, cols] = (
            jnp.dot(mixed[:, :n_cols], out_n[:, cols], preferred_element_type=F32)
            + jnp.dot(mixed[:, n_cols:], out_b[:, cols], preferred_element_type=F32)
        ).astype(BF16)

    each(0, model // tile, project)
    first = []
    for d in range(1, peers):
        peer = lax.rem(me_tp + d, peers)
        copy = remote(
            part.at[pl.ds(pl.multiple_of(peer * rows, rows), rows)], inbox.at[d - 1],
            tp_send.at[d - 1], tp_recv.at[d - 1], (me, peer),
        )
        launch(copy)
        first.append(copy)
    relay_block(0, along - 1)
    spread_block(1, 1)
    for copy in first:
        copy.wait_recv()
    total = part[pl.ds(pl.multiple_of(me_tp * rows, rows), rows), :].astype(F32)
    for d in range(1, peers):
        total = total + inbox[d - 1].astype(F32)
    updated[...] = residual[...].astype(F32) + total
    value = updated[...]
    scale = lax.rsqrt(jnp.mean(value * value, axis=-1, keepdims=True) + 1e-06)

    def rows_of(zz, cc):
        return pl.ds(pl.multiple_of((cc * along + zz) * rows, rows), rows)

    normed_all[rows_of(z, c), :] = (value * scale * gain[...]).astype(BF16)

    def pass_rows(dz, dc, via):
        held = normed_all.at[rows_of(turn(z, along - dz, along) if via else z, c)]
        return remote(
            held, held, n_send.at[dz, dc], n_recv.at[dz, dc],
            place(dc=dc) if via else place(dz=dz, dc=dc),
        )

    for dz in range(1, along):
        launch(pass_rows(dz, 0, False))
    for dc in range(1, cores):
        launch(pass_rows(0, dc, False))
    relay_block(1, 0)
    spread_block(1, 2)
    relay_block(1, 1)
    for dz in range(1, along):
        pass_rows(dz, 0, False).wait_recv()
        for dc in range(1, cores):
            launch(pass_rows(dz, dc, True))
    spread_block(1, 3) if along > 3 else None
    finish_weights(0)
    for dz in range(along):
        for dc in range(1, cores):
            pass_rows(dz, dc, dz > 0).wait_recv()

    def climb(i):
        product = jnp.dot(normed_all[...], up_buf[i], preferred_element_type=F32)
        cols = pl.ds(pl.multiple_of(i * unit, unit), unit)
        hidden[:, cols] = jnp.square(jnp.maximum(product, 0.0)).astype(BF16)

    each(0, peers, climb)
    for dz in range(2, along):
        relay_block(1, dz)
    finish_weights(1)

    own = along * rows
    chunks = 4
    width = model // chunks
    per = width // depth

    def halves(k, dc):
        cols = pl.ds(k * width, width)
        return remote(
            half_out.at[dc - 1, :, cols], half_in.at[dc - 1, :, cols],
            h_send.at[k, dc - 1], h_recv.at[k, dc - 1], place(dc=dc),
        )

    def sums(k, dz):
        cols = pl.ds(k * width, width)
        return remote(
            rows_out.at[dz - 1, :, cols], rows_in.at[dz - 1, :, cols],
            r_send.at[k, dz - 1], r_recv.at[k, dz - 1], place(dz=dz),
        )

    def gathered(zz, cols):
        found = channel[rows_of(zz, c), cols]
        at = pl.ds(pl.multiple_of(zz * rows, rows), rows)
        for dc in range(1, cores):
            found = found + half_in[dc - 1, at, cols].astype(F32)
        return found

    def descend(k):
        def one(s):
            cols = pl.ds(pl.multiple_of((k * per + s) * depth, depth), depth)
            channel[:, cols] = jnp.dot(
                hidden[...], down_buf[k * per + s], preferred_element_type=F32
            )

        each(0, per, one)
        cols = pl.ds(k * width, width)
        for dc in range(1, cores):
            theirs = pl.ds(pl.multiple_of(turn(c, dc, cores) * own, own), own)
            half_out[dc - 1, :, cols] = channel[theirs, cols].astype(BF16)
            launch(halves(k, dc))

    def hand_on(k):
        cols = pl.ds(k * width, width)
        for dc in range(1, cores):
            halves(k, dc).wait_recv()
        for dz in range(1, along):
            rows_out[dz - 1, :, cols] = gathered(turn(z, dz, along), cols).astype(BF16)
            launch(sums(k, dz))

    for k in range(chunks):
        descend(k)
        if k:
            hand_on(k - 1)
    hand_on(chunks - 1)
    for k in range(chunks):
        cols = pl.ds(k * width, width)
        total = updated[:, cols] + gathered(z, cols)
        for dz in range(1, along):
            sums(k, dz).wait_recv()
            total = total + rows_in[dz - 1, :, cols].astype(F32)
        o_ref[:, cols] = total.astype(BF16)

    def drain(t):
        for kind in range(3):
            for way in range(2):
                hop(kind, way, t).wait_send()

    each(0, shards - 1, drain)
    for copy in started:
        copy.wait_send()


def local(
    shards, peers, order, across, cores,
    query_narrow, key_narrow, value_narrow, query_broad, key_broad, value_broad,
    offset_narrow, offset_broad, residual, out_narrow, out_broad, norm_gain, up_proj, down_proj,
):
    tok, columns = query_narrow.shape
    rows, model = residual.shape
    depth, wide = up_proj.shape
    along, lanes = shards // across, peers // cores
    group = along * cores
    unit = wide // group
    chunks = 4
    pad = 16

    def padded(offset):
        return jnp.pad(offset, ((0, pad - offset.shape[0]), (0, 0)))

    vmem = pl.BlockSpec(memory_space=pltpu.VMEM)
    anywhere = pl.BlockSpec(memory_space=pl.ANY)
    dma = pltpu.SemaphoreType.DMA
    return pl.pallas_call(
        functools.partial(kernel, shards, peers, order, across, cores),
        out_shape=jax.ShapeDtypeStruct((rows, model), BF16),
        in_specs=[vmem] * 2 + [anywhere] * 6 + [vmem] * 4 + [anywhere] * 2,
        out_specs=vmem,
        scratch_shapes=[
            pltpu.VMEM((2, shards, 2 * tok, columns), BF16),
            pltpu.VMEM((2, shards, pad, tok), BF16),
            pltpu.VMEM((group, depth, unit), BF16),
            pltpu.VMEM((wide, depth), BF16),
            pltpu.VMEM((peers, model, unit), BF16),
            pltpu.VMEM((shards, peers * unit, depth), BF16),
            pltpu.VMEM((tok, 2 * columns), BF16),
            pltpu.VMEM((tok, model), BF16),
            pltpu.VMEM((peers - 1, rows, model), BF16),
            pltpu.VMEM((rows, model), F32),
            pltpu.VMEM((group * rows, model), BF16),
            pltpu.VMEM((group * rows, peers * unit), BF16),
            pltpu.VMEM((group * rows, model), F32),
            pltpu.VMEM((cores - 1, along * rows, model), BF16),
            pltpu.VMEM((cores - 1, along * rows, model), BF16),
            pltpu.VMEM((along - 1, rows, model), BF16),
            pltpu.VMEM((along - 1, rows, model), BF16),
            dma((2, 3, shards)),
            dma((2, 3, shards)),
            dma((2, along, cores)),
            dma((2, along, cores)),
            dma((2, along, lanes, across)),
            dma((2, along, across, lanes)),
            dma((2, along, across, lanes)),
            dma((peers - 1,)),
            dma((peers - 1,)),
            dma((along, cores)),
            dma((along, cores)),
            dma((chunks, cores)),
            dma((chunks, cores)),
            dma((chunks, along)),
            dma((chunks, along)),
            dma((group + 9,)),
        ],
        compiler_params=pltpu.CompilerParams(
            collective_id=0, has_side_effects=True, vmem_limit_bytes=60 << 20
        ),
    )(
        query_narrow, query_broad, key_narrow, value_narrow, key_broad, value_broad,
        padded(offset_narrow), padded(offset_broad), residual, out_narrow, out_broad,
        norm_gain.reshape(1, -1), up_proj, down_proj,
    )


def solution(mesh):
    shards, peers = mesh.shape["sp"], mesh.shape["tp"]
    across = 1 << ((shards.bit_length() - 1) // 2)
    return jax.shard_map(
        functools.partial(local, shards, peers, tuple(ring_order(shards)), across, 2),
        mesh=mesh,
        in_specs=(
            P("sp", "tp"),
            P("sp", "tp"),
            P("sp", "tp"),
            P("sp", "tp"),
            P("sp", "tp"),
            P("sp", "tp"),
            P("tp", "sp"),
            P("tp", "sp"),
            P(("sp", "tp"), None),
            P("tp", None),
            P("tp", None),
            P(),
            P("sp", "tp"),
            P("tp", "sp"),
        ),
        out_specs=P(("sp", "tp"), None),
        check_vma=False,
    )
```

```python
import functools
import math

import jax
import jax.numpy as jnp
from jax import lax
from jax.experimental import pallas as pl
from jax.experimental.pallas import tpu as pltpu
from jax.sharding import PartitionSpec as P

NARROW_SIZE = 64
BROAD_SIZE = 128
F32 = jnp.float32
BF16 = jnp.bfloat16
LOG2E = math.log2(math.e)


def ring_order(shards):
    across = 1 << ((shards.bit_length() - 1) // 2)
    along = shards // across
    order = [z * across for z in range(along)]
    for turn, z in enumerate(reversed(range(along))):
        row = list(range(1, across))
        if turn % 2:
            row.reverse()
        order += [z * across + x for x in row]
    return order


def lookup(table, index):
    found = jnp.int32(0)
    for place, value in enumerate(table):
        found = found + jnp.where(index == place, jnp.int32(value), jnp.int32(0))
    return found


def kernel(
    shards, peers, order, across, cores, column,
    q_n, q_b, k_n, v_n, k_b, v_b, off_n, off_b, residual, out_n, out_b, gain, up, down,
    o_ref,
    up_src, down_src, up_buf, down_buf, mixed, part, inbox, updated,
    normed_all, hidden, channel, half_out, half_in, rows_out, rows_in,
    a_send, a_recv, x_send, y_send, b_recv, tp_send, tp_recv,
    n_send, n_recv, h_send, h_recv, r_send, r_recv, load_sems, attention_sems,
    *attention_scratch,
):
    tok = q_n.shape[0]
    model = part.shape[1]
    rows = residual.shape[0]
    depth, wide = up.shape
    along, lanes = shards // across, peers // cores
    group = along * cores
    unit = wide // group
    me = lax.axis_index("sp")
    me_tp = lax.axis_index("tp")
    z, x = lax.div(me, across), lax.rem(me, across)
    y, c = lax.div(me_tp, cores), lax.rem(me_tp, cores)

    def turn(value, by, size):
        return lax.rem(value + by, size)

    def place(dz=0, dx=0, dy=0, dc=0):
        return (
            turn(z, dz, along) * across + turn(x, dx, across),
            turn(y, dy, lanes) * cores + turn(c, dc, cores),
        )

    def remote(src, dst, send_sem, recv_sem, where):
        return pltpu.make_async_remote_copy(
            src_ref=src, dst_ref=dst, send_sem=send_sem, recv_sem=recv_sem,
            device_id=where, device_id_type=pl.DeviceIdType.MESH,
        )

    started = []

    def launch(copy):
        copy.start()
        started.append(copy)

    def piece(m, shard, column):
        if m == 0:
            return up_buf.at[column, pl.ds(pl.multiple_of(shard * depth, depth), depth)]
        return down_buf.at[shard, pl.ds(pl.multiple_of(column * unit, unit), unit)]

    def block(m, shard, lane):
        if m == 0:
            return up_buf.at[
                pl.ds(lane * cores, cores), pl.ds(pl.multiple_of(shard * depth, depth), depth)
            ]
        size = cores * unit
        return down_buf.at[shard, pl.ds(pl.multiple_of(lane * size, size), size)]

    mine = pl.ds(pl.multiple_of((z * cores + c) * unit, unit), unit)
    weight_loads = [
        (up.at[:, pl.ds(j * unit, unit)], up_src.at[j]) for j in range(group)
    ] + [
        (down, down_src),
        (up.at[:, mine], piece(0, me, me_tp)),
        (down.at[mine], piece(1, me, me_tp)),
    ]
    weight_loads = [
        pltpu.make_async_copy(src, dst, load_sems.at[i])
        for i, (src, dst) in enumerate(weight_loads)
    ]

    def begin(loads):
        loads = [
            pltpu.make_async_copy(src, dst, attention_sems.at[i])
            for i, (src, dst) in enumerate(loads)
        ]
        for load in loads + weight_loads:
            load.start()
        return loads

    friends = [
        place(dz=dz, dc=dc) for dz in range(along) for dc in range(cores) if dz or dc
    ]
    friends += [place(dx=dx) for dx in range(1, across)]
    friends += [place(dy=dy, dc=dc) for dy in range(1, lanes) for dc in range(cores)]

    def meet():
        barrier = pltpu.get_barrier_semaphore()
        for friend in friends:
            pl.semaphore_signal(
                barrier, inc=1, device_id=friend, device_id_type=pl.DeviceIdType.MESH
            )
        pl.semaphore_wait(barrier, len(friends))

    def each(first, last, body):
        def step(t, carry):
            body(t)
            return carry

        lax.fori_loop(first, last, step, 0)

    def exchange(m, dz, dc):
        to = turn(z, dz, along) * cores + turn(c, dc, cores)
        if m == 0:
            src = up_src.at[to]
        else:
            src = down_src.at[pl.ds(pl.multiple_of(to * unit, unit), unit)]
        return remote(
            src, piece(m, me, me_tp), a_send.at[m, dz, dc], a_recv.at[m, dz, dc],
            place(dz=dz, dc=dc),
        )

    def send_column(m, hops):
        for dz in hops:
            for dc in range(cores):
                if dz or dc:
                    launch(exchange(m, dz, dc))

    def origin(dz, bx=0):
        return turn(z, along - dz, along) * across + turn(x, bx, across)

    def along_x(m, dz, by, dx):
        held = block(m, origin(dz), turn(y, by, lanes))
        return remote(
            held, held, x_send.at[m, dz, by, dx], b_recv.at[m, dz, (across - dx) % across, by],
            place(dx=dx),
        )

    def along_y(m, dz, bx, dy):
        held = block(m, origin(dz, bx), y)
        return remote(
            held, held, y_send.at[m, dz, bx, dy], b_recv.at[m, dz, bx, (lanes - dy) % lanes],
            place(dy=dy),
        )

    def await_block(m, dz, bx, by):
        held = block(m, origin(dz, bx), turn(y, by, lanes))
        remote(
            held, held, x_send.at[m, dz, 0, 0], b_recv.at[m, dz, bx, by], place(dc=1)
        ).wait_recv()

    def spread_block(m, dz):
        for dc in range(cores):
            if dz or dc:
                exchange(m, dz, dc).wait_recv()
        for dx in range(1, across):
            launch(along_x(m, dz, 0, dx))
        for dy in range(1, lanes):
            launch(along_y(m, dz, 0, dy))

    def relay_block(m, dz):
        if dz % 2 == 0:
            for bx in range(1, across):
                await_block(m, dz, bx, 0)
                for dy in range(1, lanes):
                    launch(along_y(m, dz, bx, dy))
        else:
            for by in range(1, lanes):
                await_block(m, dz, 0, by)
                for dx in range(1, across):
                    launch(along_x(m, dz, by, dx))

    def finish_weights(m):
        for dz in range(along):
            for bx in range(across):
                for by in range(lanes):
                    if bx and by or (by if dz % 2 == 0 else bx):
                        await_block(m, dz, bx, by)

    everywhere = range(along)
    beyond = range(1, along)
    row_at = lax.broadcasted_iota(jnp.int32, (tok, tok), 0)
    col_at = lax.broadcasted_iota(jnp.int32, (tok, tok), 1)
    later = (row_at > col_at).astype(BF16)
    before = col_at < row_at

    def ring_attention():
        kv_slots, off_slots, kv_send, kv_recv = attention_scratch
        inverse = [order.index(s) for s in range(shards)]
        pos = lookup(inverse, me)
        right = lookup(order, lax.rem(pos + 1, shards))
        left = lookup(order, lax.rem(pos + shards - 1, shards))
        loads = []
        for way, (k, v, off) in enumerate(((k_n, v_n, off_n), (k_b, v_b, off_b))):
            loads += [
                (k, kv_slots.at[way, 0, pl.ds(0, tok)]),
                (v, kv_slots.at[way, 0, pl.ds(tok, tok)]),
                (off, off_slots.at[way, 0]),
            ]
        loads = begin(loads)
        meet()

        def stream(kind, way, t):
            if kind == 0:
                return off_slots.at[way, t]
            return kv_slots.at[way, t, pl.ds((kind - 1) * tok, tok)]

        def hop(kind, way, t):
            return remote(
                stream(kind, way, t), stream(kind, way, t + 1),
                kv_send.at[way, kind, t], kv_recv.at[way, kind, t],
                ((left if way else right), me_tp),
            )

        def relay(t):
            for kind in range(3):
                for way in range(2):
                    hop(kind, way, t - 1).wait_recv()
                    hop(kind, way, t).start()

        for load in loads:
            load.wait()
        for kind in range(3):
            for way in range(2):
                hop(kind, way, 0).start()
        for load in weight_loads:
            load.wait()
        each(1, shards - 1, relay)
        for kind in range(3):
            for way in range(2):
                hop(kind, way, shards - 2).wait_recv()
        for m in range(2):
            send_column(m, everywhere)
        for m in range(2):
            spread_block(m, 0)

        def head_block(way, h, size, q, at, keep_sum, diagonal):
            there = lookup(inverse, at)
            slot = lax.rem((there - pos if way else pos - there) + shards, shards)
            cols = pl.ds(h * size, size)
            keys = kv_slots[way, slot, pl.ds(0, tok), cols]
            values = kv_slots[way, slot, pl.ds(tok, tok), cols]
            offset = off_slots[way, slot].astype(F32)[h : h + 1, :]
            scores = lax.dot_general(
                q[:, cols], keys, (((1,), (1,)), ((), ())), preferred_element_type=F32
            ) * (size ** -0.5 * LOG2E) + offset * LOG2E
            weight, spent = weigh(scores, diagonal, keep_sum)
            added = jnp.dot(weight, values, preferred_element_type=F32)
            return keep_sum + spent, added

        for way, (q, size) in enumerate(((q_n, NARROW_SIZE), (q_b, BROAD_SIZE))):
            for h in range(q.shape[1] // size):
                start = head_block(way, h, size, q, me, jnp.zeros((tok, 1), F32), True)

                def sweep(at, state, way=way, h=h, size=size, q=q):
                    keep_sum, running = state
                    keep_sum, added = head_block(
                        way, h, size, q, me - 1 - at, keep_sum, False
                    )
                    return keep_sum, running + added

                _, running = lax.fori_loop(0, me, sweep, start)
                mixed[:, pl.ds(way * q.shape[1] + h * size, size)] = running.astype(BF16)
        for dz in beyond:
            spread_block(0, dz)

        def drain(t):
            for kind in range(3):
                for way in range(2):
                    hop(kind, way, t).wait_send()

        return lambda: each(0, shards - 1, drain)

    def weigh(scores, diagonal, spent_before=None):
        spent = jnp.maximum(
            scores, jnp.log2(1.0 + jnp.exp2(jnp.minimum(scores, 126.0)))
        )
        breaks = scores - spent
        if diagonal:
            spent = jnp.where(before, spent, 0.0)
        rounded = spent.astype(BF16)
        after = jnp.dot(rounded, later, preferred_element_type=F32)
        power = breaks - after
        if spent_before is not None:
            power = power - spent_before
        weight = jnp.exp2(power)
        if diagonal:
            weight = jnp.where(before, weight, 0.0)
        return weight.astype(BF16), after[:, :1] + rounded[:, :1].astype(F32)

    def column_attention():
        (
            kv_src, q_src, kv_all, q_all, masked, running, spent, back,
            kv_send, kv_recv, q_send, q_recv, over_send, over_recv, twin_send, twin_recv,
            back_send, back_recv,
        ) = attention_scratch
        parts = along // cores
        wide_part = q_src.shape[3]
        row_parts = tok // wide_part
        kinds = ((q_n, k_n, v_n, off_n, NARROW_SIZE), (q_b, k_b, v_b, off_b, BROAD_SIZE))
        loads = []
        for p in range(parts):
            cols = pl.ds(p * wide_part, wide_part)
            for kind, (q, k, v, _, _) in enumerate(kinds):
                loads += [
                    (k.at[:, cols], kv_src.at[p, kind, pl.ds(0, tok)]),
                    (v.at[:, cols], kv_src.at[p, kind, pl.ds(tok, tok)]),
                    (q.at[:, cols], q_src.at[p, kind]),
                ]
        loads = begin(loads)
        pad = kv_src.shape[2] - 2 * tok
        for p in range(parts):
            for kind, (_, _, _, off, size) in enumerate(kinds):
                per = wide_part // size
                lines = []
                for h in range(p * per, (p + 1) * per):
                    for i in range(row_parts):
                        lines.append(
                            off[h : h + 1, pl.ds(i * wide_part, wide_part)].astype(F32)
                        )
                lines.append(jnp.zeros((pad - len(lines), wide_part), F32))
                kv_src[p, kind, pl.ds(2 * tok, pad), :] = jnp.concatenate(
                    lines, axis=0
                ).astype(BF16)
        meet()

        source = lax.div(z, parts)
        share = lax.rem(z, parts)
        half = jnp.where(z >= cores, jnp.int32(1), jnp.int32(0))
        taker = jnp.where(z >= cores, along - 1 - z, z)
        shifted = []

        def at_core(zz, core):
            return (zz * across + x, y * cores + core)

        def unless(same, copy):
            @pl.when(jnp.logical_not(same))
            def _():
                copy.start()

            shifted.append((same, copy))

        for load in loads:
            load.wait()
        for p in range(parts):
            zz = c * parts + p
            for r in range(cores):
                to = turn(c, r, cores)
                same = jnp.logical_and(zz == z, to == c)
                unless(same, remote(
                    kv_src.at[p, to], kv_all.at[x, z, to], kv_send.at[p, r],
                    kv_recv.at[z], at_core(zz, to),
                ))

                @pl.when(same)
                def _(p=p, to=to):
                    kv_all[x, z, to] = kv_src[p, to]

            same = jnp.logical_and(zz == z, taker == c)
            unless(same, remote(
                q_src.at[p], q_all.at[half], q_send.at[p], q_recv.at[half],
                at_core(zz, taker),
            ))

            @pl.when(same)
            def _(p=p):
                q_all[half] = q_src[p]

        for load in weight_loads:
            load.wait()
        send_column(0, everywhere)
        send_column(1, range(1))
        spread_block(0, 0)

        def from_z(dz):
            return turn(z, along - dz, along)

        def keys(bx, dz, core):
            return kv_all.at[turn(x, bx, across), from_z(dz), core]

        def await_keys(held, sem):
            remote(held, held, kv_send.at[0, 0], sem, place(dc=1)).wait_recv()

        def to_twin(bx, dz, dc):
            held = keys(bx, dz, c)
            launch(remote(
                held, held, twin_send.at[bx, dz, dc], twin_recv.at[bx, dz, dc], place(dc=dc)
            ))

        for dz in everywhere:
            if dz:
                await_keys(keys(0, dz, c), kv_recv.at[from_z(dz)])
            else:
                @pl.when(source != c)
                def _():
                    await_keys(keys(0, 0, c), kv_recv.at[z])
            held = keys(0, dz, c)
            for dx in range(1, across):
                launch(remote(
                    held, held, over_send.at[dx, dz],
                    over_recv.at[across - dx, dz], place(dx=dx),
                ))
            for dc in range(1, cores):
                to_twin(0, dz, dc)
        for bx in range(1, across):
            for dz in everywhere:
                await_keys(keys(bx, dz, c), over_recv.at[bx, dz])
                for dc in range(1, cores):
                    to_twin(bx, dz, dc)
        spread_block(1, 0)
        for bx in range(across):
            for dz in everywhere:
                for dc in range(1, cores):
                    await_keys(
                        keys(bx, dz, turn(c, cores - dc, cores)), twin_recv.at[bx, dz, dc]
                    )

        lane = lax.broadcasted_iota(jnp.int32, (tok, wide_part), 1)

        def lanes_of(h, size):
            return jnp.logical_and(lane >= h * size, lane < (h + 1) * size)

        def block_of(bx, bz, diagonal):
            scored = []
            for kind, (_, _, _, _, size) in enumerate(kinds):
                held = kv_all.at[bx, bz, kind]
                lines = held[pl.ds(2 * tok, pad), :].astype(F32) * LOG2E
                for h in range(wide_part // size):
                    first = h * row_parts
                    offset = jnp.concatenate(
                        [lines[first + i : first + i + 1] for i in range(row_parts)], axis=1
                    )
                    scores = lax.dot_general(
                        masked[kind, h], held[pl.ds(0, tok), :], (((1,), (1,)), ((), ())),
                        preferred_element_type=F32,
                    )
                    scored.append((kind, h, scores * (size ** -0.5 * LOG2E) + offset))
            weighed = [(kind, h, *weigh(scores, diagonal)) for kind, h, scores in scored]
            for kind, (_, _, _, _, size) in enumerate(kinds):
                values = kv_all[bx, bz, kind, pl.ds(tok, tok), :]
                own = [(h, w, used) for which, h, w, used in weighed if which == kind]
                added, total = None, None
                for h, w, used in own:
                    kept = values
                    if len(own) > 1:
                        kept = jnp.where(lanes_of(h, size), values, jnp.zeros_like(values))
                    product = jnp.dot(w, kept, preferred_element_type=F32)
                    used = jnp.broadcast_to(used, (tok, wide_part))
                    added = product if added is None else added + product
                    total = used if total is None else jnp.where(lanes_of(h, size), used, total)
                if diagonal:
                    running[kind] = added
                    spent[kind] = total
                else:
                    running[kind] = running[kind] + added * jnp.exp2(-spent[kind])
                    spent[kind] = spent[kind] + total

        def sweep(zq, slot):
            shard = zq * across + x
            for kind, (_, _, _, _, size) in enumerate(kinds):
                queries = q_all[slot, kind]
                for h in range(wide_part // size):
                    masked[kind, h] = jnp.where(
                        lanes_of(h, size), queries, jnp.zeros_like(queries)
                    )
            block_of(x, zq, True)

            def one(t):
                at = shard - 1 - t
                block_of(lax.rem(at, across), lax.div(at, across), False)

            each(0, shard, one)
            same = jnp.logical_and(zq == z, source == c)
            for kind, (q, _, _, _, _) in enumerate(kinds):
                at = kind * q.shape[1] + share * wide_part
                cols = pl.ds(pl.multiple_of(at, wide_part), wide_part)
                back[slot, kind] = running[kind].astype(BF16)
                unless(same, remote(
                    back.at[slot, kind], mixed.at[:, cols], back_send.at[slot, kind],
                    back_recv.at[share, kind], at_core(zq, source),
                ))

                @pl.when(same)
                def _(kind=kind, cols=cols):
                    mixed[:, cols] = running[kind].astype(BF16)

        for slot in range(2):
            zq = c if slot == 0 else along - 1 - c

            @pl.when(jnp.logical_not(jnp.logical_and(zq == z, source == c)))
            def _(slot=slot):
                remote(
                    q_all.at[slot], q_all.at[slot], q_send.at[0], q_recv.at[slot], place(dc=1)
                ).wait_recv()

            sweep(zq, slot)
            relay_block(slot, 0)
        send_column(1, beyond)
        for dz in beyond:
            spread_block(0, dz)
        for p in range(parts):
            same = jnp.logical_and(c * parts + p == z, taker == c)

            @pl.when(jnp.logical_not(same))
            def _(p=p):
                for kind, (q, _, _, _, _) in enumerate(kinds):
                    held = mixed.at[:, pl.ds(kind * q.shape[1] + p * wide_part, wide_part)]
                    remote(
                        held, held, back_send.at[0, 0], back_recv.at[p, kind], place(dc=1)
                    ).wait_recv()

        def drain():
            for same, copy in shifted:
                @pl.when(jnp.logical_not(same))
                def _(copy=copy):
                    copy.wait_send()

        return drain

    drain = column_attention() if column else ring_attention()

    tile = min(512, model)
    n_cols = out_n.shape[0]

    def project(i):
        cols = pl.ds(pl.multiple_of(i * tile, tile), tile)
        part[:, cols] = (
            jnp.dot(mixed[:, :n_cols], out_n[:, cols], preferred_element_type=F32)
            + jnp.dot(mixed[:, n_cols:], out_b[:, cols], preferred_element_type=F32)
        ).astype(BF16)

    each(0, model // tile, project)
    first = []
    for d in range(1, peers):
        peer = lax.rem(me_tp + d, peers)
        copy = remote(
            part.at[pl.ds(pl.multiple_of(peer * rows, rows), rows)], inbox.at[d - 1],
            tp_send.at[d - 1], tp_recv.at[d - 1], (me, peer),
        )
        launch(copy)
        first.append(copy)
    for dz in range(0 if not column else 1, along):
        relay_block(0, dz)
    for copy in first:
        copy.wait_recv()
    total = part[pl.ds(pl.multiple_of(me_tp * rows, rows), rows), :].astype(F32)
    for d in range(1, peers):
        total = total + inbox[d - 1].astype(F32)
    updated[...] = residual[...].astype(F32) + total
    value = updated[...]
    scale = lax.rsqrt(jnp.mean(value * value, axis=-1, keepdims=True) + 1e-06)

    def rows_of(zz, cc):
        return pl.ds(pl.multiple_of((cc * along + zz) * rows, rows), rows)

    normed_all[rows_of(z, c), :] = (value * scale * gain[...]).astype(BF16)

    def pass_rows(dz, dc, via):
        held = normed_all.at[rows_of(turn(z, along - dz, along) if via else z, c)]
        return remote(
            held, held, n_send.at[dz, dc], n_recv.at[dz, dc],
            place(dc=dc) if via else place(dz=dz, dc=dc),
        )

    for dz in range(1, along):
        launch(pass_rows(dz, 0, False))
    for dc in range(1, cores):
        launch(pass_rows(0, dc, False))
    if not column:
        relay_block(1, 0)
    for dz in beyond:
        spread_block(1, dz)
    for dz in range(1, along):
        pass_rows(dz, 0, False).wait_recv()
        for dc in range(1, cores):
            launch(pass_rows(dz, dc, True))
    finish_weights(0)
    for dz in range(along):
        for dc in range(1, cores):
            pass_rows(dz, dc, dz > 0).wait_recv()

    def climb(i):
        product = jnp.dot(normed_all[...], up_buf[i], preferred_element_type=F32)
        cols = pl.ds(pl.multiple_of(i * unit, unit), unit)
        hidden[:, cols] = jnp.square(jnp.maximum(product, 0.0)).astype(BF16)

    each(0, peers, climb)
    for dz in beyond:
        relay_block(1, dz)
    finish_weights(1)

    own = along * rows
    chunks = 4
    width = model // chunks
    per = width // depth

    def halves(k, dc):
        cols = pl.ds(k * width, width)
        return remote(
            half_out.at[dc - 1, :, cols], half_in.at[dc - 1, :, cols],
            h_send.at[k, dc - 1], h_recv.at[k, dc - 1], place(dc=dc),
        )

    def sums(k, dz):
        cols = pl.ds(k * width, width)
        return remote(
            rows_out.at[dz - 1, :, cols], rows_in.at[dz - 1, :, cols],
            r_send.at[k, dz - 1], r_recv.at[k, dz - 1], place(dz=dz),
        )

    def gathered(zz, cols):
        found = channel[rows_of(zz, c), cols]
        at = pl.ds(pl.multiple_of(zz * rows, rows), rows)
        for dc in range(1, cores):
            found = found + half_in[dc - 1, at, cols].astype(F32)
        return found

    def descend(k):
        def one(s):
            cols = pl.ds(pl.multiple_of((k * per + s) * depth, depth), depth)
            channel[:, cols] = jnp.dot(
                hidden[...], down_buf[k * per + s], preferred_element_type=F32
            )

        each(0, per, one)
        cols = pl.ds(k * width, width)
        for dc in range(1, cores):
            theirs = pl.ds(pl.multiple_of(turn(c, dc, cores) * own, own), own)
            half_out[dc - 1, :, cols] = channel[theirs, cols].astype(BF16)
            launch(halves(k, dc))

    def hand_on(k):
        cols = pl.ds(k * width, width)
        for dc in range(1, cores):
            halves(k, dc).wait_recv()
        for dz in range(1, along):
            rows_out[dz - 1, :, cols] = gathered(turn(z, dz, along), cols).astype(BF16)
            launch(sums(k, dz))

    for k in range(chunks):
        descend(k)
        if k:
            hand_on(k - 1)
    hand_on(chunks - 1)
    for k in range(chunks):
        cols = pl.ds(k * width, width)
        total = updated[:, cols] + gathered(z, cols)
        for dz in range(1, along):
            sums(k, dz).wait_recv()
            total = total + rows_in[dz - 1, :, cols].astype(F32)
        o_ref[:, cols] = total.astype(BF16)

    drain()
    for copy in started:
        copy.wait_send()


def local(
    shards, peers, order, across, cores,
    query_narrow, key_narrow, value_narrow, query_broad, key_broad, value_broad,
    offset_narrow, offset_broad, residual, out_narrow, out_broad, norm_gain, up_proj, down_proj,
):
    tok, columns = query_narrow.shape
    rows, model = residual.shape
    depth, wide = up_proj.shape
    along, lanes = shards // across, peers // cores
    group = along * cores
    unit = wide // group
    chunks = 4
    pad = 16
    parts = max(1, along // cores)
    part_columns = columns // parts
    column = (
        along == 2 * cores
        and columns % parts == 0
        and part_columns % BROAD_SIZE == 0
        and tok % part_columns == 0
    )

    def padded(offset):
        if column:
            return offset
        return jnp.pad(offset, ((0, pad - offset.shape[0]), (0, 0)))

    vmem = pl.BlockSpec(memory_space=pltpu.VMEM)
    anywhere = pl.BlockSpec(memory_space=pl.ANY)
    dma = pltpu.SemaphoreType.DMA
    if column:
        span = 2 * tok + pad
        in_specs = [anywhere] * 6 + [vmem] * 6 + [anywhere] * 2
        attention_scratch = [
            pltpu.VMEM((parts, 2, span, part_columns), BF16),
            pltpu.VMEM((parts, 2, tok, part_columns), BF16),
            pltpu.VMEM((across, along, 2, span, part_columns), BF16),
            pltpu.VMEM((2, 2, tok, part_columns), BF16),
            pltpu.VMEM((2, part_columns // NARROW_SIZE, tok, part_columns), BF16),
            pltpu.VMEM((2, tok, part_columns), F32),
            pltpu.VMEM((2, tok, part_columns), F32),
            pltpu.VMEM((2, 2, tok, part_columns), BF16),
            dma((parts, cores)),
            dma((along,)),
            dma((parts,)),
            dma((2,)),
            dma((across, along)),
            dma((across, along)),
            dma((across, along, cores)),
            dma((across, along, cores)),
            dma((2, 2)),
            dma((parts, 2)),
        ]
    else:
        in_specs = [vmem] * 2 + [anywhere] * 6 + [vmem] * 4 + [anywhere] * 2
        attention_scratch = [
            pltpu.VMEM((2, shards, 2 * tok, columns), BF16),
            pltpu.VMEM((2, shards, pad, tok), BF16),
            dma((2, 3, shards)),
            dma((2, 3, shards)),
        ]
    return pl.pallas_call(
        functools.partial(kernel, shards, peers, order, across, cores, column),
        out_shape=jax.ShapeDtypeStruct((rows, model), BF16),
        in_specs=in_specs,
        out_specs=vmem,
        scratch_shapes=[
            pltpu.VMEM((group, depth, unit), BF16),
            pltpu.VMEM((wide, depth), BF16),
            pltpu.VMEM((peers, model, unit), BF16),
            pltpu.VMEM((shards, peers * unit, depth), BF16),
            pltpu.VMEM((tok, 2 * columns), BF16),
            pltpu.VMEM((tok, model), BF16),
            pltpu.VMEM((peers - 1, rows, model), BF16),
            pltpu.VMEM((rows, model), F32),
            pltpu.VMEM((group * rows, model), BF16),
            pltpu.VMEM((group * rows, peers * unit), BF16),
            pltpu.VMEM((group * rows, model), F32),
            pltpu.VMEM((cores - 1, along * rows, model), BF16),
            pltpu.VMEM((cores - 1, along * rows, model), BF16),
            pltpu.VMEM((along - 1, rows, model), BF16),
            pltpu.VMEM((along - 1, rows, model), BF16),
            dma((2, along, cores)),
            dma((2, along, cores)),
            dma((2, along, lanes, across)),
            dma((2, along, across, lanes)),
            dma((2, along, across, lanes)),
            dma((peers - 1,)),
            dma((peers - 1,)),
            dma((along, cores)),
            dma((along, cores)),
            dma((chunks, cores)),
            dma((chunks, cores)),
            dma((chunks, along)),
            dma((chunks, along)),
            dma((group + 3,)),
            dma((6 * max(parts, 1),)),
        ] + attention_scratch,
        compiler_params=pltpu.CompilerParams(
            collective_id=0, has_side_effects=True, vmem_limit_bytes=60 << 20
        ),
    )(
        query_narrow, query_broad, key_narrow, value_narrow, key_broad, value_broad,
        padded(offset_narrow), padded(offset_broad), residual, out_narrow, out_broad,
        norm_gain.reshape(1, -1), up_proj, down_proj,
    )


def solution(mesh):
    shards, peers = mesh.shape["sp"], mesh.shape["tp"]
    across = 1 << ((shards.bit_length() - 1) // 2)
    return jax.shard_map(
        functools.partial(local, shards, peers, tuple(ring_order(shards)), across, 2),
        mesh=mesh,
        in_specs=(
            P("sp", "tp"),
            P("sp", "tp"),
            P("sp", "tp"),
            P("sp", "tp"),
            P("sp", "tp"),
            P("sp", "tp"),
            P("tp", "sp"),
            P("tp", "sp"),
            P(("sp", "tp"), None),
            P("tp", None),
            P("tp", None),
            P(),
            P("sp", "tp"),
            P("tp", "sp"),
        ),
        out_specs=P(("sp", "tp"), None),
        check_vma=False,
    )
```

```python
import functools
import math

import jax
import jax.numpy as jnp
from jax import lax
from jax.experimental import pallas as pl
from jax.experimental.pallas import tpu as pltpu
from jax.sharding import PartitionSpec as P

NARROW_SIZE = 64
BROAD_SIZE = 128
F32 = jnp.float32
BF16 = jnp.bfloat16
LOG2E = math.log2(math.e)


def ring_order(shards):
    across = 1 << ((shards.bit_length() - 1) // 2)
    along = shards // across
    order = [z * across for z in range(along)]
    for turn, z in enumerate(reversed(range(along))):
        row = list(range(1, across))
        if turn % 2:
            row.reverse()
        order += [z * across + x for x in row]
    return order


def lookup(table, index):
    found = jnp.int32(0)
    for place, value in enumerate(table):
        found = found + jnp.where(index == place, jnp.int32(value), jnp.int32(0))
    return found


def kernel(
    shards, peers, order, across, cores, column,
    q_n, q_b, k_n, v_n, k_b, v_b, off_n, off_b, residual, out_n, out_b, gain, up, down,
    o_ref,
    up_src, down_src, up_buf, down_buf, out_all, mixed, part, twin_out, twin_in,
    lane_out, lane_in, updated,
    normed_all, hidden, channel, half_out, half_in, rows_out, rows_in,
    a_send, a_recv, x_send, y_send, b_recv, t_send, t_recv, l_send, l_recv,
    n_send, n_recv, w_send, w_recv, h_send, h_recv, r_send, r_recv, load_sems, attention_sems,
    *attention_scratch,
):
    tok = q_n.shape[0]
    model = part.shape[1]
    rows = residual.shape[0]
    depth, wide = up.shape
    along, lanes = shards // across, peers // cores
    group = along * cores
    unit = wide // group
    me = lax.axis_index("sp")
    me_tp = lax.axis_index("tp")
    z, x = lax.div(me, across), lax.rem(me, across)
    y, c = lax.div(me_tp, cores), lax.rem(me_tp, cores)

    def turn(value, by, size):
        return lax.rem(value + by, size)

    def place(dz=0, dx=0, dy=0, dc=0):
        return (
            turn(z, dz, along) * across + turn(x, dx, across),
            turn(y, dy, lanes) * cores + turn(c, dc, cores),
        )

    def remote(src, dst, send_sem, recv_sem, where):
        return pltpu.make_async_remote_copy(
            src_ref=src, dst_ref=dst, send_sem=send_sem, recv_sem=recv_sem,
            device_id=where, device_id_type=pl.DeviceIdType.MESH,
        )

    started = []

    def launch(copy):
        copy.start()
        started.append(copy)

    def piece(m, shard, column):
        if m == 0:
            return up_buf.at[column, pl.ds(pl.multiple_of(shard * depth, depth), depth)]
        return down_buf.at[shard, pl.ds(pl.multiple_of(column * unit, unit), unit)]

    far_first = sorted(range(1, along), key=lambda dz: abs(2 * dz - along))
    columns = out_n.shape[0]
    mine = pl.ds(pl.multiple_of((z * cores + c) * unit, unit), unit)
    weight_loads = [
        (up.at[:, pl.ds(j * unit, unit)], up_src.at[j]) for j in range(group)
    ] + [
        (down, down_src),
        (up.at[:, mine], piece(0, me, me_tp)),
        (down.at[mine], piece(1, me, me_tp)),
        (out_n, out_all.at[pl.ds(0, columns)]),
        (out_b, out_all.at[pl.ds(columns, columns)]),
    ]
    weight_loads = [
        pltpu.make_async_copy(src, dst, load_sems.at[i])
        for i, (src, dst) in enumerate(weight_loads)
    ]

    def begin(loads):
        loads = [
            pltpu.make_async_copy(src, dst, attention_sems.at[i])
            for i, (src, dst) in enumerate(loads)
        ]
        for load in loads + weight_loads:
            load.start()
        return loads

    friends = [
        place(dz=dz, dc=dc) for dz in range(along) for dc in range(cores) if dz or dc
    ]
    friends += [place(dx=dx) for dx in range(1, across)]
    friends += [place(dy=dy, dc=dc) for dy in range(1, lanes) for dc in range(cores)]

    def meet():
        barrier = pltpu.get_barrier_semaphore()
        for friend in friends:
            pl.semaphore_signal(
                barrier, inc=1, device_id=friend, device_id_type=pl.DeviceIdType.MESH
            )
        pl.semaphore_wait(barrier, len(friends))

    def each(first, last, body):
        def step(t, carry):
            body(t)
            return carry

        lax.fori_loop(first, last, step, 0)

    def exchange(m, dz, dc):
        to = turn(z, dz, along) * cores + turn(c, dc, cores)
        if m == 0:
            src = up_src.at[to]
        else:
            src = down_src.at[pl.ds(pl.multiple_of(to * unit, unit), unit)]
        return remote(
            src, piece(m, me, me_tp), a_send.at[m, dz, dc], a_recv.at[m, dz, dc],
            place(dz=dz, dc=dc),
        )

    def send_column(m, hops):
        for dz in hops:
            for dc in range(cores):
                if dz or dc:
                    launch(exchange(m, dz, dc))

    def origin(dz, bx=0):
        return turn(z, along - dz, along) * across + turn(x, bx, across)

    def part_of(m, dz, dc, bx, by):
        core = turn(c, cores - dc, cores)
        return piece(m, origin(dz, bx), turn(y, by, lanes) * cores + core)

    def along_x(m, dz, dc, by, dx):
        held = part_of(m, dz, dc, 0, by)
        return remote(
            held, held, x_send.at[m, dz, dc, by, dx],
            b_recv.at[m, dz, dc, (across - dx) % across, by], place(dx=dx),
        )

    def along_y(m, dz, dc, bx, dy):
        held = part_of(m, dz, dc, bx, 0)
        return remote(
            held, held, y_send.at[m, dz, dc, bx, dy],
            b_recv.at[m, dz, dc, bx, (lanes - dy) % lanes], place(dy=dy),
        )

    def await_part(m, dz, dc, bx, by):
        held = part_of(m, dz, dc, bx, by)
        remote(
            held, held, x_send.at[m, dz, dc, 0, 0], b_recv.at[m, dz, dc, bx, by], place(dc=1)
        ).wait_recv()

    arrived = set()

    def spread_part(m, dz, dc, x_too=True, y_too=True):
        if (m, dz, dc) not in arrived:
            arrived.add((m, dz, dc))
            if dz or dc:
                exchange(m, dz, dc).wait_recv()
        if x_too:
            for dx in range(1, across):
                launch(along_x(m, dz, dc, 0, dx))
        if y_too:
            for dy in range(1, lanes):
                launch(along_y(m, dz, dc, 0, dy))

    def spread_block(m, dz, x_too=True, y_too=True):
        for dc in range(cores):
            spread_part(m, dz, dc, x_too, y_too)

    def x_first(dz, dc):
        return (dz + dc) % 2 == 0

    def relay_block(m, dz):
        for dc in range(cores):
            if x_first(dz, dc):
                for bx in range(1, across):
                    await_part(m, dz, dc, bx, 0)
                    for dy in range(1, lanes):
                        launch(along_y(m, dz, dc, bx, dy))
            else:
                for by in range(1, lanes):
                    await_part(m, dz, dc, 0, by)
                    for dx in range(1, across):
                        launch(along_x(m, dz, dc, by, dx))

    def finish_block(m, dz):
        for dc in range(cores):
            for bx in range(across):
                for by in range(lanes):
                    if bx and by or (by if x_first(dz, dc) else bx):
                        await_part(m, dz, dc, bx, by)

    everywhere = range(along)
    beyond = range(1, along)
    row_at = lax.broadcasted_iota(jnp.int32, (tok, tok), 0)
    col_at = lax.broadcasted_iota(jnp.int32, (tok, tok), 1)
    later = (row_at > col_at).astype(BF16)
    before = col_at < row_at

    def ring_attention():
        kv_slots, off_slots, kv_send, kv_recv = attention_scratch
        inverse = [order.index(s) for s in range(shards)]
        pos = lookup(inverse, me)
        right = lookup(order, lax.rem(pos + 1, shards))
        left = lookup(order, lax.rem(pos + shards - 1, shards))
        loads = []
        for way, (k, v, off) in enumerate(((k_n, v_n, off_n), (k_b, v_b, off_b))):
            loads += [
                (k, kv_slots.at[way, 0, pl.ds(0, tok)]),
                (v, kv_slots.at[way, 0, pl.ds(tok, tok)]),
                (off, off_slots.at[way, 0]),
            ]
        loads = begin(loads)
        meet()

        def stream(kind, way, t):
            if kind == 0:
                return off_slots.at[way, t]
            return kv_slots.at[way, t, pl.ds((kind - 1) * tok, tok)]

        def hop(kind, way, t):
            return remote(
                stream(kind, way, t), stream(kind, way, t + 1),
                kv_send.at[way, kind, t], kv_recv.at[way, kind, t],
                ((left if way else right), me_tp),
            )

        def relay(t):
            for kind in range(3):
                for way in range(2):
                    hop(kind, way, t - 1).wait_recv()
                    hop(kind, way, t).start()

        for load in loads:
            load.wait()
        for kind in range(3):
            for way in range(2):
                hop(kind, way, 0).start()
        for load in weight_loads:
            load.wait()
        each(1, shards - 1, relay)
        for kind in range(3):
            for way in range(2):
                hop(kind, way, shards - 2).wait_recv()
        for m in range(2):
            send_column(m, range(1))
        send_column(0, beyond)
        for m in range(2):
            spread_block(m, 0)

        def head_block(way, h, size, q, at, keep_sum, diagonal):
            there = lookup(inverse, at)
            slot = lax.rem((there - pos if way else pos - there) + shards, shards)
            cols = pl.ds(h * size, size)
            keys = kv_slots[way, slot, pl.ds(0, tok), cols]
            values = kv_slots[way, slot, pl.ds(tok, tok), cols]
            offset = off_slots[way, slot].astype(F32)[h : h + 1, :]
            scores = lax.dot_general(
                q[:, cols], keys, (((1,), (1,)), ((), ())), preferred_element_type=F32
            ) * (size ** -0.5 * LOG2E) + offset * LOG2E
            weight, spent = weigh(scores, diagonal, keep_sum)
            added = jnp.dot(weight, values, preferred_element_type=F32)
            return keep_sum + spent, added

        for way, (q, size) in enumerate(((q_n, NARROW_SIZE), (q_b, BROAD_SIZE))):
            for h in range(q.shape[1] // size):
                start = head_block(way, h, size, q, me, jnp.zeros((tok, 1), F32), True)

                def sweep(at, state, way=way, h=h, size=size, q=q):
                    keep_sum, running = state
                    keep_sum, added = head_block(
                        way, h, size, q, me - 1 - at, keep_sum, False
                    )
                    return keep_sum, running + added

                _, running = lax.fori_loop(0, me, sweep, start)
                mixed[:, pl.ds(way * q.shape[1] + h * size, size)] = running.astype(BF16)
        for dz in far_first[:1]:
            spread_block(0, dz)

        def drain(t):
            for kind in range(3):
                for way in range(2):
                    hop(kind, way, t).wait_send()

        return lambda: each(0, shards - 1, drain)

    def weigh(scores, diagonal, spent_before=None):
        spent = jnp.maximum(
            scores, jnp.log2(1.0 + jnp.exp2(jnp.minimum(scores, 126.0)))
        )
        breaks = scores - spent
        if diagonal:
            spent = jnp.where(before, spent, 0.0)
        rounded = spent.astype(BF16)
        after = jnp.dot(rounded, later, preferred_element_type=F32)
        power = breaks - after
        if spent_before is not None:
            power = power - spent_before
        weight = jnp.exp2(power)
        if diagonal:
            weight = jnp.where(before, weight, 0.0)
        return weight.astype(BF16), after[:, :1] + rounded[:, :1].astype(F32)

    def column_attention():
        (
            kv_src, q_src, kv_all, q_all, masked, running, spent, back,
            kv_send, kv_recv, q_send, q_recv, over_send, over_recv, twin_send, twin_recv,
            back_send, back_recv,
        ) = attention_scratch
        parts = along // cores
        wide_part = q_src.shape[3]
        row_parts = tok // wide_part
        kinds = ((q_n, k_n, v_n, off_n, NARROW_SIZE), (q_b, k_b, v_b, off_b, BROAD_SIZE))
        loads = []
        for p in range(parts):
            cols = pl.ds(p * wide_part, wide_part)
            for kind, (q, k, v, _, _) in enumerate(kinds):
                loads += [
                    (k.at[:, cols], kv_src.at[p, kind, pl.ds(0, tok)]),
                    (v.at[:, cols], kv_src.at[p, kind, pl.ds(tok, tok)]),
                    (q.at[:, cols], q_src.at[p, kind]),
                ]
        loads = begin(loads)
        pad = kv_src.shape[2] - 2 * tok
        for p in range(parts):
            for kind, (_, _, _, off, size) in enumerate(kinds):
                per = wide_part // size
                lines = []
                for h in range(p * per, (p + 1) * per):
                    for i in range(row_parts):
                        lines.append(
                            off[h : h + 1, pl.ds(i * wide_part, wide_part)].astype(F32)
                        )
                lines.append(jnp.zeros((pad - len(lines), wide_part), F32))
                kv_src[p, kind, pl.ds(2 * tok, pad), :] = jnp.concatenate(
                    lines, axis=0
                ).astype(BF16)
        meet()

        source = lax.div(z, parts)
        share = lax.rem(z, parts)
        half = jnp.where(z >= cores, jnp.int32(1), jnp.int32(0))
        taker = jnp.where(z >= cores, along - 1 - z, z)
        shifted = []

        def at_core(zz, core):
            return (zz * across + x, y * cores + core)

        def unless(same, copy):
            @pl.when(jnp.logical_not(same))
            def _():
                copy.start()

            shifted.append((same, copy))

        for load in loads:
            load.wait()
        for p in range(parts):
            zz = c * parts + p
            for r in range(cores):
                to = turn(c, r, cores)
                same = jnp.logical_and(zz == z, to == c)
                unless(same, remote(
                    kv_src.at[p, to], kv_all.at[x, z, to], kv_send.at[p, r],
                    kv_recv.at[z], at_core(zz, to),
                ))

                @pl.when(same)
                def _(p=p, to=to):
                    kv_all[x, z, to] = kv_src[p, to]

            same = jnp.logical_and(zz == z, taker == c)
            unless(same, remote(
                q_src.at[p], q_all.at[half], q_send.at[p], q_recv.at[half],
                at_core(zz, taker),
            ))

            @pl.when(same)
            def _(p=p):
                q_all[half] = q_src[p]

        for load in weight_loads:
            load.wait()
        send_column(0, range(1))
        send_column(1, range(1))
        spread_block(0, 0)

        def from_z(dz):
            return turn(z, along - dz, along)

        def keys(bx, dz, core):
            return kv_all.at[turn(x, bx, across), from_z(dz), core]

        def await_keys(held, sem):
            remote(held, held, kv_send.at[0, 0], sem, place(dc=1)).wait_recv()

        def to_twin(bx, dz, dc):
            held = keys(bx, dz, c)
            launch(remote(
                held, held, twin_send.at[bx, dz, dc], twin_recv.at[bx, dz, dc], place(dc=dc)
            ))

        for dz in everywhere:
            if dz:
                await_keys(keys(0, dz, c), kv_recv.at[from_z(dz)])
            else:
                @pl.when(source != c)
                def _():
                    await_keys(keys(0, 0, c), kv_recv.at[z])
            held = keys(0, dz, c)
            for dx in range(1, across):
                launch(remote(
                    held, held, over_send.at[dx, dz],
                    over_recv.at[across - dx, dz], place(dx=dx),
                ))
            for dc in range(1, cores):
                to_twin(0, dz, dc)
        send_column(0, far_first[:1])
        for bx in range(1, across):
            for dz in everywhere:
                await_keys(keys(bx, dz, c), over_recv.at[bx, dz])
                for dc in range(1, cores):
                    to_twin(bx, dz, dc)
        spread_block(1, 0)
        for bx in range(across):
            for dz in everywhere:
                for dc in range(1, cores):
                    await_keys(
                        keys(bx, dz, turn(c, cores - dc, cores)), twin_recv.at[bx, dz, dc]
                    )

        lane = lax.broadcasted_iota(jnp.int32, (tok, wide_part), 1)

        def lanes_of(h, size):
            return jnp.logical_and(lane >= h * size, lane < (h + 1) * size)

        def block_of(bx, bz, diagonal):
            scored = []
            for kind, (_, _, _, _, size) in enumerate(kinds):
                held = kv_all.at[bx, bz, kind]
                lines = held[pl.ds(2 * tok, pad), :].astype(F32) * LOG2E
                for h in range(wide_part // size):
                    first = h * row_parts
                    offset = jnp.concatenate(
                        [lines[first + i : first + i + 1] for i in range(row_parts)], axis=1
                    )
                    scores = lax.dot_general(
                        masked[kind, h], held[pl.ds(0, tok), :], (((1,), (1,)), ((), ())),
                        preferred_element_type=F32,
                    )
                    scored.append((kind, h, scores * (size ** -0.5 * LOG2E) + offset))
            weighed = [(kind, h, *weigh(scores, diagonal)) for kind, h, scores in scored]
            for kind, (_, _, _, _, size) in enumerate(kinds):
                values = kv_all[bx, bz, kind, pl.ds(tok, tok), :]
                own = [(h, w, used) for which, h, w, used in weighed if which == kind]
                added, total = None, None
                for h, w, used in own:
                    kept = values
                    if len(own) > 1:
                        kept = jnp.where(lanes_of(h, size), values, jnp.zeros_like(values))
                    product = jnp.dot(w, kept, preferred_element_type=F32)
                    used = jnp.broadcast_to(used, (tok, wide_part))
                    added = product if added is None else added + product
                    total = used if total is None else jnp.where(lanes_of(h, size), used, total)
                if diagonal:
                    running[kind] = added
                    spent[kind] = total
                else:
                    running[kind] = running[kind] + added * jnp.exp2(-spent[kind])
                    spent[kind] = spent[kind] + total

        def sweep(zq, slot):
            shard = zq * across + x
            for kind, (_, _, _, _, size) in enumerate(kinds):
                queries = q_all[slot, kind]
                for h in range(wide_part // size):
                    masked[kind, h] = jnp.where(
                        lanes_of(h, size), queries, jnp.zeros_like(queries)
                    )
            block_of(x, zq, True)

            def one(t):
                at = shard - 1 - t
                block_of(lax.rem(at, across), lax.div(at, across), False)

            each(0, shard, one)
            same = jnp.logical_and(zq == z, source == c)
            for kind, (q, _, _, _, _) in enumerate(kinds):
                at = kind * q.shape[1] + share * wide_part
                cols = pl.ds(pl.multiple_of(at, wide_part), wide_part)
                back[slot, kind] = running[kind].astype(BF16)
                unless(same, remote(
                    back.at[slot, kind], mixed.at[:, cols], back_send.at[slot, kind],
                    back_recv.at[share, kind], at_core(zq, source),
                ))

                @pl.when(same)
                def _(kind=kind, cols=cols):
                    mixed[:, cols] = running[kind].astype(BF16)

        for slot in range(2):
            zq = c if slot == 0 else along - 1 - c

            @pl.when(jnp.logical_not(jnp.logical_and(zq == z, source == c)))
            def _(slot=slot):
                remote(
                    q_all.at[slot], q_all.at[slot], q_send.at[0], q_recv.at[slot], place(dc=1)
                ).wait_recv()

            sweep(zq, slot)
            relay_block(slot, 0)
        send_column(0, far_first[1:2])
        for dz in far_first[:1]:
            spread_block(0, dz)
        for p in range(parts):
            same = jnp.logical_and(c * parts + p == z, taker == c)

            @pl.when(jnp.logical_not(same))
            def _(p=p):
                for kind, (q, _, _, _, _) in enumerate(kinds):
                    held = mixed.at[:, pl.ds(kind * q.shape[1] + p * wide_part, wide_part)]
                    remote(
                        held, held, back_send.at[0, 0], back_recv.at[p, kind], place(dc=1)
                    ).wait_recv()

        send_column(0, far_first[2:])
        send_column(1, far_first[:1])

        def drain():
            for same, copy in shifted:
                @pl.when(jnp.logical_not(same))
                def _(copy=copy):
                    copy.wait_send()

        return drain

    drain = column_attention() if column else ring_attention()

    chunks = 4
    width = model // chunks

    def chunk(k):
        return pl.ds(k * width, width)

    def twins(k, dc):
        return remote(
            twin_out.at[dc - 1, :, chunk(k)], twin_in.at[dc - 1, :, chunk(k)],
            t_send.at[k, dc - 1], t_recv.at[k, dc - 1], place(dc=dc),
        )

    def others(k, dy):
        return remote(
            lane_out.at[dy - 1, :, chunk(k)], lane_in.at[dy - 1, :, chunk(k)],
            l_send.at[k, dy - 1], l_recv.at[k, dy - 1], place(dy=dy),
        )

    def part_rows(lane, core):
        return pl.ds(pl.multiple_of((lane * cores + core) * rows, rows), rows)

    def paired(lane, k):
        found = part[part_rows(lane, c), chunk(k)]
        at = pl.ds(pl.multiple_of(lane * rows, rows), rows)
        for dc in range(1, cores):
            found = found + twin_in[dc - 1, at, chunk(k)].astype(F32)
        return found

    for k in range(chunks):
        part[:, chunk(k)] = jnp.dot(
            mixed[...], out_all[:, chunk(k)], preferred_element_type=F32
        )
        for dc in range(1, cores):
            for lane in range(lanes):
                twin_out[dc - 1, pl.ds(lane * rows, rows), chunk(k)] = part[
                    part_rows(lane, turn(c, dc, cores)), chunk(k)
                ].astype(BF16)
            launch(twins(k, dc))
    for k in range(chunks):
        for dc in range(1, cores):
            twins(k, dc).wait_recv()
        for dy in range(1, lanes):
            lane_out[dy - 1, :, chunk(k)] = paired(turn(y, dy, lanes), k).astype(BF16)
            launch(others(k, dy))
    if not column:
        relay_block(0, 0)
        relay_block(1, 0)
    for dz in far_first[:1]:
        relay_block(0, dz)
    for dz in far_first[1:2]:
        spread_block(0, dz, y_too=False)
    for k in range(chunks):
        total = residual[:, chunk(k)].astype(F32) + paired(y, k)
        for dy in range(1, lanes):
            others(k, dy).wait_recv()
            total = total + lane_in[dy - 1, :, chunk(k)].astype(F32)
        updated[:, chunk(k)] = total
    value = updated[...]
    scale = lax.rsqrt(jnp.mean(value * value, axis=-1, keepdims=True) + 1e-06)

    def rows_of(zz, cc):
        return pl.ds(pl.multiple_of((cc * along + zz) * rows, rows), rows)

    normed_all[rows_of(z, c), :] = (value * scale * gain[...]).astype(BF16)

    def rows_at(zz):
        return normed_all.at[rows_of(zz, c)]

    def pass_line(zz, way, step):
        to = z + (-1 if way else 1)
        return remote(
            rows_at(zz), rows_at(zz), n_send.at[way, step], n_recv.at[way, step],
            (to * across + x, me_tp),
        )

    def pass_twin(zz, way, step, dc):
        return remote(
            rows_at(zz), rows_at(zz), w_send.at[way, step, dc], w_recv.at[way, step, dc],
            place(dc=dc),
        )

    chained = []

    def when(wanted, copy):
        @pl.when(wanted)
        def _():
            copy.start()

        chained.append((wanted, copy))

    def can_go(way):
        return z > 0 if way else z < along - 1

    for way in range(2):
        when(can_go(way), pass_line(z, way, 0))
    for dc in range(1, cores):
        launch(pass_twin(z, 0, 0, dc))

    def follow(step):
        for way in range(2):
            zz = z + step if way else z - step
            there = zz < along if way else zz >= 0

            @pl.when(there)
            def _(way=way, zz=zz):
                pass_line(zz, way, step - 1).wait_recv()

            if step < along - 1:
                when(jnp.logical_and(there, can_go(way)), pass_line(zz, way, step))
            for dc in range(1, cores):
                when(there, pass_twin(zz, way, step, dc))

    send_column(1, far_first[1:])
    for dz in far_first[1:2]:
        spread_block(0, dz, x_too=False)
    for dz in far_first[2:]:
        spread_block(0, dz)
    for dz in far_first[1:]:
        relay_block(0, dz)
    for step in beyond:
        follow(step)
    for dz in far_first[:1]:
        spread_block(1, dz)
    for dz in everywhere:
        finish_block(0, dz)
    for dc in range(1, cores):
        pass_twin(z, 0, 0, dc).wait_recv()
        for step in beyond:
            for way in range(2):
                zz = z + step if way else z - step

                @pl.when(zz < along if way else zz >= 0)
                def _(way=way, zz=zz, step=step, dc=dc):
                    pass_twin(zz, way, step, dc).wait_recv()

    def climb(i):
        product = jnp.dot(normed_all[...], up_buf[i], preferred_element_type=F32)
        cols = pl.ds(pl.multiple_of(i * unit, unit), unit)
        hidden[:, cols] = jnp.square(jnp.maximum(product, 0.0)).astype(BF16)

    each(0, peers, climb)
    own = along * rows
    strip = model // along

    def strip_of(dz):
        start = turn(z, along - dz, along) * strip
        return pl.ds(pl.multiple_of(start, strip), strip)

    def halves(k, dc):
        return remote(
            half_out.at[dc - 1, :, strip_of(k)], half_in.at[dc - 1, :, strip_of(k)],
            h_send.at[k, dc - 1], h_recv.at[k, dc - 1], place(dc=dc),
        )

    def sums(k, dz):
        return remote(
            rows_out.at[dz - 1, :, strip_of(k)], rows_in.at[dz - 1, :, strip_of(k)],
            r_send.at[k, dz - 1], r_recv.at[k, dz - 1], place(dz=dz),
        )

    def gathered(zz, cols):
        found = channel[rows_of(zz, c), cols]
        at = pl.ds(pl.multiple_of(zz * rows, rows), rows)
        for dc in range(1, cores):
            found = found + half_in[dc - 1, at, cols].astype(F32)
        return found

    def descend(k):
        finish_block(1, k)

        def one(i):
            shard = origin(k) - x + i
            cols = pl.ds(pl.multiple_of(shard * depth, depth), depth)
            channel[:, cols] = jnp.dot(
                hidden[...], down_buf[shard], preferred_element_type=F32
            )

        each(0, across, one)
        cols = strip_of(k)
        for dc in range(1, cores):
            theirs = pl.ds(pl.multiple_of(turn(c, dc, cores) * own, own), own)
            half_out[dc - 1, :, cols] = channel[theirs, cols].astype(BF16)
            launch(halves(k, dc))

    def hand_on(k):
        cols = strip_of(k)
        for dc in range(1, cores):
            halves(k, dc).wait_recv()
        for dz in far_first:
            rows_out[dz - 1, :, cols] = gathered(turn(z, dz, along), cols).astype(BF16)
            launch(sums(k, dz))

    descend(0)
    for dz in far_first[:1]:
        relay_block(1, dz)
    hand_on(0)
    for dz in far_first[1:]:
        spread_block(1, dz)
    last = 0
    for dz in far_first:
        if dz not in far_first[:1]:
            relay_block(1, dz)
        descend(dz)
        if last:
            hand_on(last)
        last = dz
    hand_on(last)
    for k in everywhere:
        for dz in range(1, along):
            sums(k, dz).wait_recv()
    for k in everywhere:
        cols = pl.ds(k * strip, strip)
        total = updated[:, cols] + gathered(z, cols)
        for dz in range(1, along):
            total = total + rows_in[dz - 1, :, cols].astype(F32)
        o_ref[:, cols] = total.astype(BF16)

    drain()
    for wanted, copy in chained:
        @pl.when(wanted)
        def _(copy=copy):
            copy.wait_send()

    for copy in started:
        copy.wait_send()


def local(
    shards, peers, order, across, cores,
    query_narrow, key_narrow, value_narrow, query_broad, key_broad, value_broad,
    offset_narrow, offset_broad, residual, out_narrow, out_broad, norm_gain, up_proj, down_proj,
):
    tok, columns = query_narrow.shape
    rows, model = residual.shape
    depth, wide = up_proj.shape
    along, lanes = shards // across, peers // cores
    group = along * cores
    unit = wide // group
    chunks = 4
    pad = 16
    parts = max(1, along // cores)
    part_columns = columns // parts
    column = (
        along == 2 * cores
        and columns % parts == 0
        and part_columns % BROAD_SIZE == 0
        and tok % part_columns == 0
    )

    def padded(offset):
        if column:
            return offset
        return jnp.pad(offset, ((0, pad - offset.shape[0]), (0, 0)))

    vmem = pl.BlockSpec(memory_space=pltpu.VMEM)
    anywhere = pl.BlockSpec(memory_space=pl.ANY)
    dma = pltpu.SemaphoreType.DMA
    if column:
        span = 2 * tok + pad
        in_specs = [anywhere] * 6 + [vmem] * 3 + [anywhere] * 2 + [vmem] + [anywhere] * 2
        attention_scratch = [
            pltpu.VMEM((parts, 2, span, part_columns), BF16),
            pltpu.VMEM((parts, 2, tok, part_columns), BF16),
            pltpu.VMEM((across, along, 2, span, part_columns), BF16),
            pltpu.VMEM((2, 2, tok, part_columns), BF16),
            pltpu.VMEM((2, part_columns // NARROW_SIZE, tok, part_columns), BF16),
            pltpu.VMEM((2, tok, part_columns), F32),
            pltpu.VMEM((2, tok, part_columns), F32),
            pltpu.VMEM((2, 2, tok, part_columns), BF16),
            dma((parts, cores)),
            dma((along,)),
            dma((parts,)),
            dma((2,)),
            dma((across, along)),
            dma((across, along)),
            dma((across, along, cores)),
            dma((across, along, cores)),
            dma((2, 2)),
            dma((parts, 2)),
        ]
    else:
        in_specs = [vmem] * 2 + [anywhere] * 6 + [vmem] + [anywhere] * 2 + [vmem] + [anywhere] * 2
        attention_scratch = [
            pltpu.VMEM((2, shards, 2 * tok, columns), BF16),
            pltpu.VMEM((2, shards, pad, tok), BF16),
            dma((2, 3, shards)),
            dma((2, 3, shards)),
        ]
    return pl.pallas_call(
        functools.partial(kernel, shards, peers, order, across, cores, column),
        out_shape=jax.ShapeDtypeStruct((rows, model), BF16),
        in_specs=in_specs,
        out_specs=vmem,
        scratch_shapes=[
            pltpu.VMEM((group, depth, unit), BF16),
            pltpu.VMEM((wide, depth), BF16),
            pltpu.VMEM((peers, model, unit), BF16),
            pltpu.VMEM((shards, peers * unit, depth), BF16),
            pltpu.VMEM((2 * columns, model), BF16),
            pltpu.VMEM((tok, 2 * columns), BF16),
            pltpu.VMEM((tok, model), F32),
            pltpu.VMEM((cores - 1, lanes * rows, model), BF16),
            pltpu.VMEM((cores - 1, lanes * rows, model), BF16),
            pltpu.VMEM((lanes - 1, rows, model), BF16),
            pltpu.VMEM((lanes - 1, rows, model), BF16),
            pltpu.VMEM((rows, model), F32),
            pltpu.VMEM((group * rows, model), BF16),
            pltpu.VMEM((group * rows, peers * unit), BF16),
            pltpu.VMEM((group * rows, model), F32),
            pltpu.VMEM((cores - 1, along * rows, model), BF16),
            pltpu.VMEM((cores - 1, along * rows, model), BF16),
            pltpu.VMEM((along - 1, rows, model), BF16),
            pltpu.VMEM((along - 1, rows, model), BF16),
            dma((2, along, cores)),
            dma((2, along, cores)),
            dma((2, along, cores, lanes, across)),
            dma((2, along, cores, across, lanes)),
            dma((2, along, cores, across, lanes)),
            dma((chunks, cores)),
            dma((chunks, cores)),
            dma((chunks, lanes)),
            dma((chunks, lanes)),
            dma((2, along)),
            dma((2, along)),
            dma((2, along, cores)),
            dma((2, along, cores)),
            dma((along, cores)),
            dma((along, cores)),
            dma((along, along)),
            dma((along, along)),
            dma((group + 5,)),
            dma((6 * max(parts, 1),)),
        ] + attention_scratch,
        compiler_params=pltpu.CompilerParams(
            collective_id=0, has_side_effects=True, vmem_limit_bytes=60 << 20
        ),
    )(
        query_narrow, query_broad, key_narrow, value_narrow, key_broad, value_broad,
        padded(offset_narrow), padded(offset_broad), residual, out_narrow, out_broad,
        norm_gain.reshape(1, -1), up_proj, down_proj,
    )


def solution(mesh):
    shards, peers = mesh.shape["sp"], mesh.shape["tp"]
    across = 1 << ((shards.bit_length() - 1) // 2)
    return jax.shard_map(
        functools.partial(local, shards, peers, tuple(ring_order(shards)), across, 2),
        mesh=mesh,
        in_specs=(
            P("sp", "tp"),
            P("sp", "tp"),
            P("sp", "tp"),
            P("sp", "tp"),
            P("sp", "tp"),
            P("sp", "tp"),
            P("tp", "sp"),
            P("tp", "sp"),
            P(("sp", "tp"), None),
            P("tp", None),
            P("tp", None),
            P(),
            P("sp", "tp"),
            P("tp", "sp"),
        ),
        out_specs=P(("sp", "tp"), None),
        check_vma=False,
    )
```

```python
import functools
import math

import jax
import jax.numpy as jnp
from jax import lax
from jax.experimental import pallas as pl
from jax.experimental.pallas import tpu as pltpu
from jax.sharding import PartitionSpec as P

NARROW_SIZE = 64
BROAD_SIZE = 128
F32 = jnp.float32
BF16 = jnp.bfloat16
LOG2E = math.log2(math.e)


def ring_order(shards):
    across = 1 << ((shards.bit_length() - 1) // 2)
    along = shards // across
    order = [z * across for z in range(along)]
    for turn, z in enumerate(reversed(range(along))):
        row = list(range(1, across))
        if turn % 2:
            row.reverse()
        order += [z * across + x for x in row]
    return order


def lookup(table, index):
    found = jnp.int32(0)
    for place, value in enumerate(table):
        found = found + jnp.where(index == place, jnp.int32(value), jnp.int32(0))
    return found


def kernel(
    shards, peers, order, across, cores, column,
    q_n, q_b, k_n, v_n, k_b, v_b, off_n, off_b, residual, out_n, out_b, gain, up, down,
    o_ref,
    up_src, down_src, up_buf, down_buf, out_all, mixed, part, twin_out, twin_in,
    lane_out, lane_in, updated,
    normed_all, hidden, channel, half_out, half_in, rows_out, rows_in,
    a_send, a_recv, x_send, y_send, b_recv, t_send, t_recv, l_send, l_recv,
    n_send, n_recv, w_send, w_recv, h_send, h_recv, r_send, r_recv, load_sems, attention_sems,
    *attention_scratch,
):
    tok = q_n.shape[0]
    model = part.shape[1]
    rows = residual.shape[0]
    depth, wide = up.shape
    along, lanes = shards // across, peers // cores
    group = along * cores
    unit = wide // group
    me = lax.axis_index("sp")
    me_tp = lax.axis_index("tp")
    z, x = lax.div(me, across), lax.rem(me, across)
    y, c = lax.div(me_tp, cores), lax.rem(me_tp, cores)

    def turn(value, by, size):
        return lax.rem(value + by, size)

    def place(dz=0, dx=0, dy=0, dc=0):
        return (
            turn(z, dz, along) * across + turn(x, dx, across),
            turn(y, dy, lanes) * cores + turn(c, dc, cores),
        )

    def remote(src, dst, send_sem, recv_sem, where):
        return pltpu.make_async_remote_copy(
            src_ref=src, dst_ref=dst, send_sem=send_sem, recv_sem=recv_sem,
            device_id=where, device_id_type=pl.DeviceIdType.MESH,
        )

    started = []

    def launch(copy):
        copy.start()
        started.append(copy)

    def piece(m, shard, column):
        if m == 0:
            return up_buf.at[column, pl.ds(pl.multiple_of(shard * depth, depth), depth)]
        return down_buf.at[shard, pl.ds(pl.multiple_of(column * unit, unit), unit)]

    far_first = sorted(range(1, along), key=lambda dz: abs(2 * dz - along))
    columns = out_n.shape[0]
    mine = pl.ds(pl.multiple_of((z * cores + c) * unit, unit), unit)
    weight_loads = [
        (up.at[:, pl.ds(j * unit, unit)], up_src.at[j]) for j in range(group)
    ] + [
        (down, down_src),
        (up.at[:, mine], piece(0, me, me_tp)),
        (down.at[mine], piece(1, me, me_tp)),
        (out_n, out_all.at[pl.ds(0, columns)]),
        (out_b, out_all.at[pl.ds(columns, columns)]),
    ]
    weight_loads = [
        pltpu.make_async_copy(src, dst, load_sems.at[i])
        for i, (src, dst) in enumerate(weight_loads)
    ]

    def begin(loads):
        loads = [
            pltpu.make_async_copy(src, dst, attention_sems.at[i])
            for i, (src, dst) in enumerate(loads)
        ]
        for load in loads + weight_loads:
            load.start()
        return loads

    friends = [
        place(dz=dz, dc=dc) for dz in range(along) for dc in range(cores) if dz or dc
    ]
    friends += [place(dx=dx) for dx in range(1, across)]
    friends += [place(dy=dy, dc=dc) for dy in range(1, lanes) for dc in range(cores)]

    def meet():
        barrier = pltpu.get_barrier_semaphore()
        for friend in friends:
            pl.semaphore_signal(
                barrier, inc=1, device_id=friend, device_id_type=pl.DeviceIdType.MESH
            )
        pl.semaphore_wait(barrier, len(friends))

    def each(first, last, body):
        def step(t, carry):
            body(t)
            return carry

        lax.fori_loop(first, last, step, 0)

    def exchange(m, dz, dc):
        to = turn(z, dz, along) * cores + turn(c, dc, cores)
        if m == 0:
            src = up_src.at[to]
        else:
            src = down_src.at[pl.ds(pl.multiple_of(to * unit, unit), unit)]
        return remote(
            src, piece(m, me, me_tp), a_send.at[m, dz, dc], a_recv.at[m, dz, dc],
            place(dz=dz, dc=dc),
        )

    def send_column(m, hops):
        for dz in hops:
            for dc in range(cores):
                if dz or dc:
                    launch(exchange(m, dz, dc))

    def origin(dz, bx=0):
        return turn(z, along - dz, along) * across + turn(x, bx, across)

    def part_of(m, dz, dc, bx, by):
        core = turn(c, cores - dc, cores)
        return piece(m, origin(dz, bx), turn(y, by, lanes) * cores + core)

    def along_x(m, dz, dc, by, dx):
        held = part_of(m, dz, dc, 0, by)
        return remote(
            held, held, x_send.at[m, dz, dc, by, dx],
            b_recv.at[m, dz, dc, (across - dx) % across, by], place(dx=dx),
        )

    def along_y(m, dz, dc, bx, dy):
        held = part_of(m, dz, dc, bx, 0)
        return remote(
            held, held, y_send.at[m, dz, dc, bx, dy],
            b_recv.at[m, dz, dc, bx, (lanes - dy) % lanes], place(dy=dy),
        )

    def await_part(m, dz, dc, bx, by):
        held = part_of(m, dz, dc, bx, by)
        remote(
            held, held, x_send.at[m, dz, dc, 0, 0], b_recv.at[m, dz, dc, bx, by], place(dc=1)
        ).wait_recv()

    arrived = set()

    def spread_part(m, dz, dc, x_too=True, y_too=True):
        if (m, dz, dc) not in arrived:
            arrived.add((m, dz, dc))
            if dz or dc:
                exchange(m, dz, dc).wait_recv()
        if x_too:
            for dx in range(1, across):
                launch(along_x(m, dz, dc, 0, dx))
        if y_too:
            for dy in range(1, lanes):
                launch(along_y(m, dz, dc, 0, dy))

    def spread_block(m, dz, x_too=True, y_too=True):
        for dc in range(cores):
            spread_part(m, dz, dc, x_too, y_too)

    def x_first(dz, dc):
        return (dz + dc) % 2 == 0

    def relay_block(m, dz):
        for dc in range(cores):
            if x_first(dz, dc):
                for bx in range(1, across):
                    await_part(m, dz, dc, bx, 0)
                    for dy in range(1, lanes):
                        launch(along_y(m, dz, dc, bx, dy))
            else:
                for by in range(1, lanes):
                    await_part(m, dz, dc, 0, by)
                    for dx in range(1, across):
                        launch(along_x(m, dz, dc, by, dx))

    def finish_block(m, dz):
        for dc in range(cores):
            for bx in range(across):
                for by in range(lanes):
                    if bx and by or (by if x_first(dz, dc) else bx):
                        await_part(m, dz, dc, bx, by)

    everywhere = range(along)
    beyond = range(1, along)
    row_at = lax.broadcasted_iota(jnp.int32, (tok, tok), 0)
    col_at = lax.broadcasted_iota(jnp.int32, (tok, tok), 1)
    later = (row_at > col_at).astype(BF16)
    before = col_at < row_at

    def ring_attention():
        kv_slots, off_slots, kv_send, kv_recv = attention_scratch
        inverse = [order.index(s) for s in range(shards)]
        pos = lookup(inverse, me)
        right = lookup(order, lax.rem(pos + 1, shards))
        left = lookup(order, lax.rem(pos + shards - 1, shards))
        loads = []
        for way, (k, v, off) in enumerate(((k_n, v_n, off_n), (k_b, v_b, off_b))):
            loads += [
                (k, kv_slots.at[way, 0, pl.ds(0, tok)]),
                (v, kv_slots.at[way, 0, pl.ds(tok, tok)]),
                (off, off_slots.at[way, 0]),
            ]
        loads = begin(loads)
        meet()

        def stream(kind, way, t):
            if kind == 0:
                return off_slots.at[way, t]
            return kv_slots.at[way, t, pl.ds((kind - 1) * tok, tok)]

        def hop(kind, way, t):
            return remote(
                stream(kind, way, t), stream(kind, way, t + 1),
                kv_send.at[way, kind, t], kv_recv.at[way, kind, t],
                ((left if way else right), me_tp),
            )

        def relay(t):
            for kind in range(3):
                for way in range(2):
                    hop(kind, way, t - 1).wait_recv()
                    hop(kind, way, t).start()

        for load in loads:
            load.wait()
        for kind in range(3):
            for way in range(2):
                hop(kind, way, 0).start()
        for load in weight_loads:
            load.wait()
        each(1, shards - 1, relay)
        for kind in range(3):
            for way in range(2):
                hop(kind, way, shards - 2).wait_recv()
        for m in range(2):
            send_column(m, range(1))
        send_column(0, beyond)
        for m in range(2):
            spread_block(m, 0)

        def head_block(way, h, size, q, at, keep_sum, diagonal):
            there = lookup(inverse, at)
            slot = lax.rem((there - pos if way else pos - there) + shards, shards)
            cols = pl.ds(h * size, size)
            keys = kv_slots[way, slot, pl.ds(0, tok), cols]
            values = kv_slots[way, slot, pl.ds(tok, tok), cols]
            offset = off_slots[way, slot].astype(F32)[h : h + 1, :]
            scores = lax.dot_general(
                q[:, cols], keys, (((1,), (1,)), ((), ())), preferred_element_type=F32
            ) * (size ** -0.5 * LOG2E) + offset * LOG2E
            weight, spent = weigh(scores, diagonal, keep_sum)
            added = jnp.dot(weight, values, preferred_element_type=F32)
            return keep_sum + spent, added

        for way, (q, size) in enumerate(((q_n, NARROW_SIZE), (q_b, BROAD_SIZE))):
            for h in range(q.shape[1] // size):
                start = head_block(way, h, size, q, me, jnp.zeros((tok, 1), F32), True)

                def sweep(at, state, way=way, h=h, size=size, q=q):
                    keep_sum, running = state
                    keep_sum, added = head_block(
                        way, h, size, q, me - 1 - at, keep_sum, False
                    )
                    return keep_sum, running + added

                _, running = lax.fori_loop(0, me, sweep, start)
                mixed[:, pl.ds(way * q.shape[1] + h * size, size)] = running.astype(BF16)
        for dz in far_first[:1]:
            spread_block(0, dz)

        def drain(t):
            for kind in range(3):
                for way in range(2):
                    hop(kind, way, t).wait_send()

        return lambda: each(0, shards - 1, drain)

    def weigh(scores, diagonal, spent_before=None):
        spent = jnp.maximum(
            scores, jnp.log2(1.0 + jnp.exp2(jnp.minimum(scores, 126.0)))
        )
        breaks = scores - spent
        if diagonal:
            spent = jnp.where(before, spent, 0.0)
        rounded = spent.astype(BF16)
        after = jnp.dot(rounded, later, preferred_element_type=F32)
        power = breaks - after
        if spent_before is not None:
            power = power - spent_before
        weight = jnp.exp2(power)
        if diagonal:
            weight = jnp.where(before, weight, 0.0)
        return weight.astype(BF16), after[:, :1] + rounded[:, :1].astype(F32)

    def column_attention():
        (
            kv_src, q_src, kv_all, q_all, masked, running, spent, back,
            kv_send, kv_recv, q_send, q_recv, over_send, over_recv, twin_send, twin_recv,
            back_send, back_recv,
        ) = attention_scratch
        parts = along // cores
        wide_part = q_src.shape[3]
        row_parts = tok // wide_part
        kinds = ((q_n, k_n, v_n, off_n, NARROW_SIZE), (q_b, k_b, v_b, off_b, BROAD_SIZE))
        loads = []
        for p in range(parts):
            cols = pl.ds(p * wide_part, wide_part)
            for kind, (q, k, v, _, _) in enumerate(kinds):
                loads += [
                    (k.at[:, cols], kv_src.at[p, kind, pl.ds(0, tok)]),
                    (v.at[:, cols], kv_src.at[p, kind, pl.ds(tok, tok)]),
                    (q.at[:, cols], q_src.at[p, kind]),
                ]
        loads = begin(loads)
        pad = kv_src.shape[2] - 2 * tok
        for p in range(parts):
            for kind, (_, _, _, off, size) in enumerate(kinds):
                per = wide_part // size
                lines = []
                for h in range(p * per, (p + 1) * per):
                    for i in range(row_parts):
                        lines.append(
                            off[h : h + 1, pl.ds(i * wide_part, wide_part)].astype(F32)
                        )
                lines.append(jnp.zeros((pad - len(lines), wide_part), F32))
                kv_src[p, kind, pl.ds(2 * tok, pad), :] = jnp.concatenate(
                    lines, axis=0
                ).astype(BF16)
        meet()

        source = lax.div(z, parts)
        share = lax.rem(z, parts)
        half = jnp.where(z >= cores, jnp.int32(1), jnp.int32(0))
        taker = jnp.where(z >= cores, along - 1 - z, z)
        shifted = []

        def at_core(zz, core):
            return (zz * across + x, y * cores + core)

        def unless(same, copy):
            @pl.when(jnp.logical_not(same))
            def _():
                copy.start()

            shifted.append((same, copy))

        for load in loads:
            load.wait()
        for p in range(parts):
            zz = c * parts + p
            for r in range(cores):
                to = turn(c, r, cores)
                same = jnp.logical_and(zz == z, to == c)
                unless(same, remote(
                    kv_src.at[p, to], kv_all.at[x, z, to], kv_send.at[p, r],
                    kv_recv.at[z], at_core(zz, to),
                ))

                @pl.when(same)
                def _(p=p, to=to):
                    kv_all[x, z, to] = kv_src[p, to]

            same = jnp.logical_and(zz == z, taker == c)
            unless(same, remote(
                q_src.at[p], q_all.at[half], q_send.at[p], q_recv.at[half],
                at_core(zz, taker),
            ))

            @pl.when(same)
            def _(p=p):
                q_all[half] = q_src[p]

        for load in weight_loads:
            load.wait()
        send_column(0, range(1))
        send_column(1, range(1))
        spread_block(0, 0)

        def from_z(dz):
            return turn(z, along - dz, along)

        def keys(bx, dz, core):
            return kv_all.at[turn(x, bx, across), from_z(dz), core]

        def await_keys(held, sem):
            remote(held, held, kv_send.at[0, 0], sem, place(dc=1)).wait_recv()

        def to_twin(bx, dz, dc):
            held = keys(bx, dz, c)
            launch(remote(
                held, held, twin_send.at[bx, dz, dc], twin_recv.at[bx, dz, dc], place(dc=dc)
            ))

        for dz in everywhere:
            if dz:
                await_keys(keys(0, dz, c), kv_recv.at[from_z(dz)])
            else:
                @pl.when(source != c)
                def _():
                    await_keys(keys(0, 0, c), kv_recv.at[z])
            held = keys(0, dz, c)
            for dx in range(1, across):
                launch(remote(
                    held, held, over_send.at[dx, dz],
                    over_recv.at[across - dx, dz], place(dx=dx),
                ))
            for dc in range(1, cores):
                to_twin(0, dz, dc)
        send_column(0, far_first[:1])
        for bx in range(1, across):
            for dz in everywhere:
                await_keys(keys(bx, dz, c), over_recv.at[bx, dz])
                for dc in range(1, cores):
                    to_twin(bx, dz, dc)
        spread_block(1, 0)
        for bx in range(across):
            for dz in everywhere:
                for dc in range(1, cores):
                    await_keys(
                        keys(bx, dz, turn(c, cores - dc, cores)), twin_recv.at[bx, dz, dc]
                    )

        lane = lax.broadcasted_iota(jnp.int32, (tok, wide_part), 1)

        def lanes_of(h, size):
            return jnp.logical_and(lane >= h * size, lane < (h + 1) * size)

        def block_of(bx, bz, diagonal):
            scored = []
            for kind, (_, _, _, _, size) in enumerate(kinds):
                held = kv_all.at[bx, bz, kind]
                lines = held[pl.ds(2 * tok, pad), :].astype(F32) * LOG2E
                for h in range(wide_part // size):
                    first = h * row_parts
                    offset = jnp.concatenate(
                        [lines[first + i : first + i + 1] for i in range(row_parts)], axis=1
                    )
                    scores = lax.dot_general(
                        masked[kind, h], held[pl.ds(0, tok), :], (((1,), (1,)), ((), ())),
                        preferred_element_type=F32,
                    )
                    scored.append((kind, h, scores * (size ** -0.5 * LOG2E) + offset))
            weighed = [(kind, h, *weigh(scores, diagonal)) for kind, h, scores in scored]
            for kind, (_, _, _, _, size) in enumerate(kinds):
                values = kv_all[bx, bz, kind, pl.ds(tok, tok), :]
                own = [(h, w, used) for which, h, w, used in weighed if which == kind]
                added, total = None, None
                for h, w, used in own:
                    kept = values
                    if len(own) > 1:
                        kept = jnp.where(lanes_of(h, size), values, jnp.zeros_like(values))
                    product = jnp.dot(w, kept, preferred_element_type=F32)
                    used = jnp.broadcast_to(used, (tok, wide_part))
                    added = product if added is None else added + product
                    total = used if total is None else jnp.where(lanes_of(h, size), used, total)
                if diagonal:
                    running[kind] = added
                    spent[kind] = total
                else:
                    running[kind] = running[kind] + added * jnp.exp2(-spent[kind])
                    spent[kind] = spent[kind] + total

        def sweep(zq, slot):
            shard = zq * across + x
            for kind, (_, _, _, _, size) in enumerate(kinds):
                queries = q_all[slot, kind]
                for h in range(wide_part // size):
                    masked[kind, h] = jnp.where(
                        lanes_of(h, size), queries, jnp.zeros_like(queries)
                    )
            block_of(x, zq, True)

            def one(t):
                at = shard - 1 - t
                block_of(lax.rem(at, across), lax.div(at, across), False)

            each(0, shard, one)
            same = jnp.logical_and(zq == z, source == c)
            for kind, (q, _, _, _, _) in enumerate(kinds):
                at = kind * q.shape[1] + share * wide_part
                cols = pl.ds(pl.multiple_of(at, wide_part), wide_part)
                back[slot, kind] = running[kind].astype(BF16)
                unless(same, remote(
                    back.at[slot, kind], mixed.at[:, cols], back_send.at[slot, kind],
                    back_recv.at[share, kind], at_core(zq, source),
                ))

                @pl.when(same)
                def _(kind=kind, cols=cols):
                    mixed[:, cols] = running[kind].astype(BF16)

        for slot in range(2):
            zq = c if slot == 0 else along - 1 - c

            @pl.when(jnp.logical_not(jnp.logical_and(zq == z, source == c)))
            def _(slot=slot):
                remote(
                    q_all.at[slot], q_all.at[slot], q_send.at[0], q_recv.at[slot], place(dc=1)
                ).wait_recv()

            sweep(zq, slot)
            relay_block(slot, 0)
        send_column(0, far_first[1:2])
        for dz in far_first[:1]:
            spread_block(0, dz)
        for p in range(parts):
            same = jnp.logical_and(c * parts + p == z, taker == c)

            @pl.when(jnp.logical_not(same))
            def _(p=p):
                for kind, (q, _, _, _, _) in enumerate(kinds):
                    held = mixed.at[:, pl.ds(kind * q.shape[1] + p * wide_part, wide_part)]
                    remote(
                        held, held, back_send.at[0, 0], back_recv.at[p, kind], place(dc=1)
                    ).wait_recv()

        send_column(0, far_first[2:])
        send_column(1, far_first[:1])

        def drain():
            for same, copy in shifted:
                @pl.when(jnp.logical_not(same))
                def _(copy=copy):
                    copy.wait_send()

        return drain

    drain = column_attention() if column else ring_attention()

    chunks = 4
    width = model // chunks

    def chunk(k):
        return pl.ds(k * width, width)

    def twins(k, dc):
        return remote(
            twin_out.at[dc - 1, :, chunk(k)], twin_in.at[dc - 1, :, chunk(k)],
            t_send.at[k, dc - 1], t_recv.at[k, dc - 1], place(dc=dc),
        )

    def others(k, dy):
        return remote(
            lane_out.at[dy - 1, :, chunk(k)], lane_in.at[dy - 1, :, chunk(k)],
            l_send.at[k, dy - 1], l_recv.at[k, dy - 1], place(dy=dy),
        )

    def part_rows(lane, core):
        return pl.ds(pl.multiple_of((lane * cores + core) * rows, rows), rows)

    def paired(lane, k):
        found = part[part_rows(lane, c), chunk(k)]
        at = pl.ds(pl.multiple_of(lane * rows, rows), rows)
        for dc in range(1, cores):
            found = found + twin_in[dc - 1, at, chunk(k)].astype(F32)
        return found

    for k in range(chunks):
        part[:, chunk(k)] = jnp.dot(
            mixed[...], out_all[:, chunk(k)], preferred_element_type=F32
        )
        for dc in range(1, cores):
            for lane in range(lanes):
                twin_out[dc - 1, pl.ds(lane * rows, rows), chunk(k)] = part[
                    part_rows(lane, turn(c, dc, cores)), chunk(k)
                ].astype(BF16)
            launch(twins(k, dc))
    for k in range(chunks):
        for dc in range(1, cores):
            twins(k, dc).wait_recv()
        for dy in range(1, lanes):
            lane_out[dy - 1, :, chunk(k)] = paired(turn(y, dy, lanes), k).astype(BF16)
            launch(others(k, dy))
    if not column:
        relay_block(0, 0)
        relay_block(1, 0)
    for dz in far_first[:1]:
        relay_block(0, dz)
    for dz in far_first[1:2]:
        spread_block(0, dz, y_too=False)
    for k in range(chunks):
        total = residual[:, chunk(k)].astype(F32) + paired(y, k)
        for dy in range(1, lanes):
            others(k, dy).wait_recv()
            total = total + lane_in[dy - 1, :, chunk(k)].astype(F32)
        updated[:, chunk(k)] = total
    value = updated[...]
    scale = lax.rsqrt(jnp.mean(value * value, axis=-1, keepdims=True) + 1e-06)

    def rows_of(zz, cc):
        return pl.ds(pl.multiple_of((zz * cores + cc) * rows, rows), rows)

    normed_all[rows_of(z, c), :] = (value * scale * gain[...]).astype(BF16)

    def rows_at(zz):
        return normed_all.at[rows_of(zz, c)]

    def pass_line(zz, way, step):
        to = z + (-1 if way else 1)
        return remote(
            rows_at(zz), rows_at(zz), n_send.at[way, step], n_recv.at[way, step],
            (to * across + x, me_tp),
        )

    def pass_twin(zz, way, step, dc):
        return remote(
            rows_at(zz), rows_at(zz), w_send.at[way, step, dc], w_recv.at[way, step, dc],
            place(dc=dc),
        )

    chained = []

    def when(wanted, copy):
        @pl.when(wanted)
        def _():
            copy.start()

        chained.append((wanted, copy))

    def can_go(way):
        return z > 0 if way else z < along - 1

    for way in range(2):
        when(can_go(way), pass_line(z, way, 0))
    for dc in range(1, cores):
        launch(pass_twin(z, 0, 0, dc))

    def follow(step):
        for way in range(2):
            zz = z + step if way else z - step
            there = zz < along if way else zz >= 0

            @pl.when(there)
            def _(way=way, zz=zz):
                pass_line(zz, way, step - 1).wait_recv()

            if step < along - 1:
                when(jnp.logical_and(there, can_go(way)), pass_line(zz, way, step))
            for dc in range(1, cores):
                when(there, pass_twin(zz, way, step, dc))

    for dz in far_first[1:2]:
        spread_block(0, dz, x_too=False)
    for dz in far_first[2:]:
        spread_block(0, dz)
    def climb(zz):
        slab = pl.ds(pl.multiple_of(zz * cores * rows, cores * rows), cores * rows)

        def one(i):
            product = jnp.dot(normed_all[slab, :], up_buf[i], preferred_element_type=F32)
            cols = pl.ds(pl.multiple_of(i * unit, unit), unit)
            hidden[slab, cols] = jnp.square(jnp.maximum(product, 0.0)).astype(BF16)

        each(0, peers, one)

    def climb_step(step):
        def side(way):
            zz = jnp.where(way == 1, z + step, z - step)

            @pl.when(jnp.logical_and(zz >= 0, zz < along))
            def _():
                for dc in range(1, cores):
                    pass_twin(zz, way, step, dc).wait_recv()
                climb(zz)

        each(0, 2, side)

    def pass_on(step):
        follow(step)
        send_column(1, far_first[step : step + 1])

    pass_on(1)
    for dz in far_first[1:]:
        relay_block(0, dz)
    for dz in far_first[:1]:
        spread_block(1, dz)
    for step in beyond[1:-1]:
        pass_on(step)
    for dz in far_first[1:2]:
        spread_block(1, dz)
    for dz in far_first[:1]:
        relay_block(1, dz)
    for dz in everywhere:
        finish_block(0, dz)
    for dc in range(1, cores):
        pass_twin(z, 0, 0, dc).wait_recv()
    climb(z)
    climb_step(1)
    for step in beyond[1:-1]:
        climb_step(step)
    for step in beyond[1:][-1:]:
        pass_on(step)
    for dz in far_first[1:2]:
        relay_block(1, dz)
    for dz in far_first[2:]:
        spread_block(1, dz)
    for step in beyond[1:][-1:]:
        climb_step(step)

    strip = model // along

    def strip_of(dz):
        start = turn(z, along - dz, along) * strip
        return pl.ds(pl.multiple_of(start, strip), strip)

    def halves(k, dc):
        return remote(
            half_out.at[dc - 1, :, strip_of(k)], half_in.at[dc - 1, :, strip_of(k)],
            h_send.at[k, dc - 1], h_recv.at[k, dc - 1], place(dc=dc),
        )

    def sums(k, dz):
        return remote(
            rows_out.at[dz - 1, :, strip_of(k)], rows_in.at[dz - 1, :, strip_of(k)],
            r_send.at[k, dz - 1], r_recv.at[k, dz - 1], place(dz=dz),
        )

    def gathered(zz, cols):
        found = channel[rows_of(zz, c), cols]
        at = pl.ds(pl.multiple_of(zz * rows, rows), rows)
        for dc in range(1, cores):
            found = found + half_in[dc - 1, at, cols].astype(F32)
        return found

    def descend(k):
        finish_block(1, k)

        def one(i):
            shard = origin(k) - x + i
            cols = pl.ds(pl.multiple_of(shard * depth, depth), depth)
            channel[:, cols] = jnp.dot(
                hidden[...], down_buf[shard], preferred_element_type=F32
            )

        each(0, across, one)
        cols = strip_of(k)
        for dc in range(1, cores):
            for zz in everywhere:
                half_out[dc - 1, pl.ds(zz * rows, rows), cols] = channel[
                    rows_of(zz, turn(c, dc, cores)), cols
                ].astype(BF16)
            launch(halves(k, dc))

    def hand_on(k):
        cols = strip_of(k)
        for dc in range(1, cores):
            halves(k, dc).wait_recv()
        for dz in far_first:
            rows_out[dz - 1, :, cols] = gathered(turn(z, dz, along), cols).astype(BF16)
            launch(sums(k, dz))

    descend(0)
    last = 0
    for i, dz in enumerate(far_first):
        if i > 1:
            relay_block(1, dz)
        descend(dz)
        hand_on(last)
        last = dz
    hand_on(last)
    for k in everywhere:
        for dz in range(1, along):
            sums(k, dz).wait_recv()
    for k in everywhere:
        cols = pl.ds(k * strip, strip)
        total = updated[:, cols] + gathered(z, cols)
        for dz in range(1, along):
            total = total + rows_in[dz - 1, :, cols].astype(F32)
        o_ref[:, cols] = total.astype(BF16)

    drain()
    for wanted, copy in chained:
        @pl.when(wanted)
        def _(copy=copy):
            copy.wait_send()

    for copy in started:
        copy.wait_send()


def local(
    shards, peers, order, across, cores,
    query_narrow, key_narrow, value_narrow, query_broad, key_broad, value_broad,
    offset_narrow, offset_broad, residual, out_narrow, out_broad, norm_gain, up_proj, down_proj,
):
    tok, columns = query_narrow.shape
    rows, model = residual.shape
    depth, wide = up_proj.shape
    along, lanes = shards // across, peers // cores
    group = along * cores
    unit = wide // group
    chunks = 4
    pad = 16
    parts = max(1, along // cores)
    part_columns = columns // parts
    column = (
        along == 2 * cores
        and columns % parts == 0
        and part_columns % BROAD_SIZE == 0
        and tok % part_columns == 0
    )

    def padded(offset):
        if column:
            return offset
        return jnp.pad(offset, ((0, pad - offset.shape[0]), (0, 0)))

    vmem = pl.BlockSpec(memory_space=pltpu.VMEM)
    anywhere = pl.BlockSpec(memory_space=pl.ANY)
    dma = pltpu.SemaphoreType.DMA
    if column:
        span = 2 * tok + pad
        in_specs = [anywhere] * 6 + [vmem] * 3 + [anywhere] * 2 + [vmem] + [anywhere] * 2
        attention_scratch = [
            pltpu.VMEM((parts, 2, span, part_columns), BF16),
            pltpu.VMEM((parts, 2, tok, part_columns), BF16),
            pltpu.VMEM((across, along, 2, span, part_columns), BF16),
            pltpu.VMEM((2, 2, tok, part_columns), BF16),
            pltpu.VMEM((2, part_columns // NARROW_SIZE, tok, part_columns), BF16),
            pltpu.VMEM((2, tok, part_columns), F32),
            pltpu.VMEM((2, tok, part_columns), F32),
            pltpu.VMEM((2, 2, tok, part_columns), BF16),
            dma((parts, cores)),
            dma((along,)),
            dma((parts,)),
            dma((2,)),
            dma((across, along)),
            dma((across, along)),
            dma((across, along, cores)),
            dma((across, along, cores)),
            dma((2, 2)),
            dma((parts, 2)),
        ]
    else:
        in_specs = [vmem] * 2 + [anywhere] * 6 + [vmem] + [anywhere] * 2 + [vmem] + [anywhere] * 2
        attention_scratch = [
            pltpu.VMEM((2, shards, 2 * tok, columns), BF16),
            pltpu.VMEM((2, shards, pad, tok), BF16),
            dma((2, 3, shards)),
            dma((2, 3, shards)),
        ]
    return pl.pallas_call(
        functools.partial(kernel, shards, peers, order, across, cores, column),
        out_shape=jax.ShapeDtypeStruct((rows, model), BF16),
        in_specs=in_specs,
        out_specs=vmem,
        scratch_shapes=[
            pltpu.VMEM((group, depth, unit), BF16),
            pltpu.VMEM((wide, depth), BF16),
            pltpu.VMEM((peers, model, unit), BF16),
            pltpu.VMEM((shards, peers * unit, depth), BF16),
            pltpu.VMEM((2 * columns, model), BF16),
            pltpu.VMEM((tok, 2 * columns), BF16),
            pltpu.VMEM((tok, model), F32),
            pltpu.VMEM((cores - 1, lanes * rows, model), BF16),
            pltpu.VMEM((cores - 1, lanes * rows, model), BF16),
            pltpu.VMEM((lanes - 1, rows, model), BF16),
            pltpu.VMEM((lanes - 1, rows, model), BF16),
            pltpu.VMEM((rows, model), F32),
            pltpu.VMEM((group * rows, model), BF16),
            pltpu.VMEM((group * rows, peers * unit), BF16),
            pltpu.VMEM((group * rows, model), F32),
            pltpu.VMEM((cores - 1, along * rows, model), BF16),
            pltpu.VMEM((cores - 1, along * rows, model), BF16),
            pltpu.VMEM((along - 1, rows, model), BF16),
            pltpu.VMEM((along - 1, rows, model), BF16),
            dma((2, along, cores)),
            dma((2, along, cores)),
            dma((2, along, cores, lanes, across)),
            dma((2, along, cores, across, lanes)),
            dma((2, along, cores, across, lanes)),
            dma((chunks, cores)),
            dma((chunks, cores)),
            dma((chunks, lanes)),
            dma((chunks, lanes)),
            dma((2, along)),
            dma((2, along)),
            dma((2, along, cores)),
            dma((2, along, cores)),
            dma((along, cores)),
            dma((along, cores)),
            dma((along, along)),
            dma((along, along)),
            dma((group + 5,)),
            dma((6 * max(parts, 1),)),
        ] + attention_scratch,
        compiler_params=pltpu.CompilerParams(
            collective_id=0, has_side_effects=True, vmem_limit_bytes=60 << 20
        ),
    )(
        query_narrow, query_broad, key_narrow, value_narrow, key_broad, value_broad,
        padded(offset_narrow), padded(offset_broad), residual, out_narrow, out_broad,
        norm_gain.reshape(1, -1), up_proj, down_proj,
    )


def solution(mesh):
    shards, peers = mesh.shape["sp"], mesh.shape["tp"]
    across = 1 << ((shards.bit_length() - 1) // 2)
    return jax.shard_map(
        functools.partial(local, shards, peers, tuple(ring_order(shards)), across, 2),
        mesh=mesh,
        in_specs=(
            P("sp", "tp"),
            P("sp", "tp"),
            P("sp", "tp"),
            P("sp", "tp"),
            P("sp", "tp"),
            P("sp", "tp"),
            P("tp", "sp"),
            P("tp", "sp"),
            P(("sp", "tp"), None),
            P("tp", None),
            P("tp", None),
            P(),
            P("sp", "tp"),
            P("tp", "sp"),
        ),
        out_specs=P(("sp", "tp"), None),
        check_vma=False,
    )
```

```python
import functools
import math

import jax
import jax.numpy as jnp
from jax import lax
from jax.experimental import pallas as pl
from jax.experimental.pallas import tpu as pltpu
from jax.sharding import PartitionSpec as P

NARROW_SIZE = 64
BROAD_SIZE = 128
F32 = jnp.float32
BF16 = jnp.bfloat16
LOG2E = math.log2(math.e)


def ring_order(shards):
    across = 1 << ((shards.bit_length() - 1) // 2)
    along = shards // across
    order = [z * across for z in range(along)]
    for turn, z in enumerate(reversed(range(along))):
        row = list(range(1, across))
        if turn % 2:
            row.reverse()
        order += [z * across + x for x in row]
    return order


def lookup(table, index):
    found = jnp.int32(0)
    for place, value in enumerate(table):
        found = found + jnp.where(index == place, jnp.int32(value), jnp.int32(0))
    return found


def kernel(
    shards, peers, order, across, cores, column,
    q_n, q_b, k_n, v_n, k_b, v_b, off_n, off_b, residual, out_n, out_b, gain, up, down,
    o_ref,
    up_src, down_src, up_buf, down_buf, out_all, mixed, part, twin_out, twin_in,
    lane_out, lane_in, updated,
    normed_all, hidden, channel, half_out, half_in, rows_out, rows_in,
    a_send, a_recv, x_send, y_send, b_recv, t_send, t_recv, l_send, l_recv,
    n_send, n_recv, w_send, w_recv, h_send, h_recv, r_send, r_recv, load_sems, attention_sems,
    *attention_scratch,
):
    tok = q_n.shape[0]
    model = part.shape[1]
    rows = residual.shape[0]
    depth, wide = up.shape
    along, lanes = shards // across, peers // cores
    group = along * cores
    unit = wide // group
    me = lax.axis_index("sp")
    me_tp = lax.axis_index("tp")
    z, x = lax.div(me, across), lax.rem(me, across)
    y, c = lax.div(me_tp, cores), lax.rem(me_tp, cores)

    def turn(value, by, size):
        return lax.rem(value + by, size)

    def place(dz=0, dx=0, dy=0, dc=0):
        return (
            turn(z, dz, along) * across + turn(x, dx, across),
            turn(y, dy, lanes) * cores + turn(c, dc, cores),
        )

    def remote(src, dst, send_sem, recv_sem, where):
        return pltpu.make_async_remote_copy(
            src_ref=src, dst_ref=dst, send_sem=send_sem, recv_sem=recv_sem,
            device_id=where, device_id_type=pl.DeviceIdType.MESH,
        )

    started = []

    def launch(copy):
        copy.start()
        started.append(copy)

    def piece(m, shard, column):
        if m == 0:
            return up_buf.at[column, pl.ds(pl.multiple_of(shard * depth, depth), depth)]
        return down_buf.at[shard, pl.ds(pl.multiple_of(column * unit, unit), unit)]

    far_first = sorted(range(1, along), key=lambda dz: abs(2 * dz - along))
    columns = out_n.shape[0]
    mine = pl.ds(pl.multiple_of((z * cores + c) * unit, unit), unit)
    weight_loads = [
        (up.at[:, pl.ds(j * unit, unit)], up_src.at[j]) for j in range(group)
    ] + [
        (down, down_src),
        (up.at[:, mine], piece(0, me, me_tp)),
        (down.at[mine], piece(1, me, me_tp)),
        (out_n, out_all.at[pl.ds(0, columns)]),
        (out_b, out_all.at[pl.ds(columns, columns)]),
    ]
    weight_loads = [
        pltpu.make_async_copy(src, dst, load_sems.at[i])
        for i, (src, dst) in enumerate(weight_loads)
    ]

    def begin(loads):
        loads = [
            pltpu.make_async_copy(src, dst, attention_sems.at[i])
            for i, (src, dst) in enumerate(loads)
        ]
        for load in loads + weight_loads:
            load.start()
        return loads

    friends = [
        place(dz=dz, dc=dc) for dz in range(along) for dc in range(cores) if dz or dc
    ]
    friends += [place(dx=dx) for dx in range(1, across)]
    friends += [place(dy=dy, dc=dc) for dy in range(1, lanes) for dc in range(cores)]

    def meet():
        barrier = pltpu.get_barrier_semaphore()
        for friend in friends:
            pl.semaphore_signal(
                barrier, inc=1, device_id=friend, device_id_type=pl.DeviceIdType.MESH
            )
        pl.semaphore_wait(barrier, len(friends))

    def each(first, last, body):
        def step(t, carry):
            body(t)
            return carry

        lax.fori_loop(first, last, step, 0)

    def exchange(m, dz, dc):
        to = turn(z, dz, along) * cores + turn(c, dc, cores)
        if m == 0:
            src = up_src.at[to]
        else:
            src = down_src.at[pl.ds(pl.multiple_of(to * unit, unit), unit)]
        return remote(
            src, piece(m, me, me_tp), a_send.at[m, dz, dc], a_recv.at[m, dz, dc],
            place(dz=dz, dc=dc),
        )

    def send_column(m, hops):
        for dz in hops:
            for dc in range(cores):
                if dz or dc:
                    launch(exchange(m, dz, dc))

    def origin(dz, bx=0):
        return turn(z, along - dz, along) * across + turn(x, bx, across)

    def part_of(m, dz, dc, bx, by):
        core = turn(c, cores - dc, cores)
        return piece(m, origin(dz, bx), turn(y, by, lanes) * cores + core)

    def along_x(m, dz, dc, by, dx):
        held = part_of(m, dz, dc, 0, by)
        return remote(
            held, held, x_send.at[m, dz, dc, by, dx],
            b_recv.at[m, dz, dc, (across - dx) % across, by], place(dx=dx),
        )

    def along_y(m, dz, dc, bx, dy):
        held = part_of(m, dz, dc, bx, 0)
        return remote(
            held, held, y_send.at[m, dz, dc, bx, dy],
            b_recv.at[m, dz, dc, bx, (lanes - dy) % lanes], place(dy=dy),
        )

    def await_part(m, dz, dc, bx, by):
        held = part_of(m, dz, dc, bx, by)
        remote(
            held, held, x_send.at[m, dz, dc, 0, 0], b_recv.at[m, dz, dc, bx, by], place(dc=1)
        ).wait_recv()

    arrived = set()

    def spread_part(m, dz, dc, x_too=True, y_too=True):
        if (m, dz, dc) not in arrived:
            arrived.add((m, dz, dc))
            if dz or dc:
                exchange(m, dz, dc).wait_recv()
        if x_too:
            for dx in range(1, across):
                launch(along_x(m, dz, dc, 0, dx))
        if y_too:
            for dy in range(1, lanes):
                launch(along_y(m, dz, dc, 0, dy))

    def spread_block(m, dz, x_too=True, y_too=True):
        for dc in range(cores):
            spread_part(m, dz, dc, x_too, y_too)

    def x_first(dz, dc):
        return (dz + dc) % 2 == 0

    def relay_block(m, dz):
        for dc in range(cores):
            if x_first(dz, dc):
                for bx in range(1, across):
                    await_part(m, dz, dc, bx, 0)
                    for dy in range(1, lanes):
                        launch(along_y(m, dz, dc, bx, dy))
            else:
                for by in range(1, lanes):
                    await_part(m, dz, dc, 0, by)
                    for dx in range(1, across):
                        launch(along_x(m, dz, dc, by, dx))

    def finish_block(m, dz):
        for dc in range(cores):
            for bx in range(across):
                for by in range(lanes):
                    if bx and by or (by if x_first(dz, dc) else bx):
                        await_part(m, dz, dc, bx, by)

    everywhere = range(along)
    beyond = range(1, along)
    row_at = lax.broadcasted_iota(jnp.int32, (tok, tok), 0)
    col_at = lax.broadcasted_iota(jnp.int32, (tok, tok), 1)
    later = (row_at > col_at).astype(BF16)
    before = col_at < row_at

    def ring_attention():
        kv_slots, off_slots, kv_send, kv_recv = attention_scratch
        inverse = [order.index(s) for s in range(shards)]
        pos = lookup(inverse, me)
        right = lookup(order, lax.rem(pos + 1, shards))
        left = lookup(order, lax.rem(pos + shards - 1, shards))
        loads = []
        for way, (k, v, off) in enumerate(((k_n, v_n, off_n), (k_b, v_b, off_b))):
            loads += [
                (k, kv_slots.at[way, 0, pl.ds(0, tok)]),
                (v, kv_slots.at[way, 0, pl.ds(tok, tok)]),
                (off, off_slots.at[way, 0]),
            ]
        loads = begin(loads)
        meet()

        def stream(kind, way, t):
            if kind == 0:
                return off_slots.at[way, t]
            return kv_slots.at[way, t, pl.ds((kind - 1) * tok, tok)]

        def hop(kind, way, t):
            return remote(
                stream(kind, way, t), stream(kind, way, t + 1),
                kv_send.at[way, kind, t], kv_recv.at[way, kind, t],
                ((left if way else right), me_tp),
            )

        def relay(t):
            for kind in range(3):
                for way in range(2):
                    hop(kind, way, t - 1).wait_recv()
                    hop(kind, way, t).start()

        for load in loads:
            load.wait()
        for kind in range(3):
            for way in range(2):
                hop(kind, way, 0).start()
        for load in weight_loads:
            load.wait()
        each(1, shards - 1, relay)
        for kind in range(3):
            for way in range(2):
                hop(kind, way, shards - 2).wait_recv()
        for m in range(2):
            send_column(m, range(1))
        send_column(0, beyond)
        for m in range(2):
            spread_block(m, 0)

        def head_block(way, h, size, q, at, keep_sum, diagonal):
            there = lookup(inverse, at)
            slot = lax.rem((there - pos if way else pos - there) + shards, shards)
            cols = pl.ds(h * size, size)
            keys = kv_slots[way, slot, pl.ds(0, tok), cols]
            values = kv_slots[way, slot, pl.ds(tok, tok), cols]
            offset = off_slots[way, slot].astype(F32)[h : h + 1, :]
            scores = lax.dot_general(
                q[:, cols], keys, (((1,), (1,)), ((), ())), preferred_element_type=F32
            ) * (size ** -0.5 * LOG2E) + offset * LOG2E
            weight, spent = weigh(scores, diagonal, keep_sum)
            added = jnp.dot(weight, values, preferred_element_type=F32)
            return keep_sum + spent, added

        for way, (q, size) in enumerate(((q_n, NARROW_SIZE), (q_b, BROAD_SIZE))):
            for h in range(q.shape[1] // size):
                start = head_block(way, h, size, q, me, jnp.zeros((tok, 1), F32), True)

                def sweep(at, state, way=way, h=h, size=size, q=q):
                    keep_sum, running = state
                    keep_sum, added = head_block(
                        way, h, size, q, me - 1 - at, keep_sum, False
                    )
                    return keep_sum, running + added

                _, running = lax.fori_loop(0, me, sweep, start)
                mixed[:, pl.ds(way * q.shape[1] + h * size, size)] = running.astype(BF16)
        for dz in far_first[:1]:
            spread_block(0, dz)

        def drain(t):
            for kind in range(3):
                for way in range(2):
                    hop(kind, way, t).wait_send()

        return lambda: each(0, shards - 1, drain)

    def weigh(scores, diagonal, spent_before=None):
        spent = jnp.maximum(
            scores, jnp.log2(1.0 + jnp.exp2(jnp.minimum(scores, 126.0)))
        )
        breaks = scores - spent
        if diagonal:
            spent = jnp.where(before, spent, 0.0)
        rounded = spent.astype(BF16)
        after = jnp.dot(rounded, later, preferred_element_type=F32)
        power = breaks - after
        if spent_before is not None:
            power = power - spent_before
        weight = jnp.exp2(power)
        if diagonal:
            weight = jnp.where(before, weight, 0.0)
        return weight.astype(BF16), after[:, :1] + rounded[:, :1].astype(F32)

    def column_attention():
        (
            kv_src, q_src, kv_all, q_all, masked, running, spent, back,
            kv_send, kv_recv, q_send, q_recv, over_send, over_recv, twin_send, twin_recv,
            back_send, back_recv,
        ) = attention_scratch
        parts = along // cores
        wide_part = q_src.shape[3]
        row_parts = tok // wide_part
        kinds = ((q_n, k_n, v_n, off_n, NARROW_SIZE), (q_b, k_b, v_b, off_b, BROAD_SIZE))
        loads = []
        for p in range(parts):
            cols = pl.ds(p * wide_part, wide_part)
            for kind, (q, k, v, _, _) in enumerate(kinds):
                loads += [
                    (k.at[:, cols], kv_src.at[p, kind, pl.ds(0, tok)]),
                    (v.at[:, cols], kv_src.at[p, kind, pl.ds(tok, tok)]),
                    (q.at[:, cols], q_src.at[p, kind]),
                ]
        loads = begin(loads)
        pad = kv_src.shape[2] - 2 * tok
        for p in range(parts):
            for kind, (_, _, _, off, size) in enumerate(kinds):
                per = wide_part // size
                lines = []
                for h in range(p * per, (p + 1) * per):
                    for i in range(row_parts):
                        lines.append(
                            off[h : h + 1, pl.ds(i * wide_part, wide_part)].astype(F32)
                        )
                lines.append(jnp.zeros((pad - len(lines), wide_part), F32))
                kv_src[p, kind, pl.ds(2 * tok, pad), :] = jnp.concatenate(
                    lines, axis=0
                ).astype(BF16)
        meet()

        source = lax.div(z, parts)
        share = lax.rem(z, parts)
        half = jnp.where(z >= cores, jnp.int32(1), jnp.int32(0))
        taker = jnp.where(z >= cores, along - 1 - z, z)
        shifted = []

        def at_core(zz, core):
            return (zz * across + x, y * cores + core)

        def unless(same, copy):
            @pl.when(jnp.logical_not(same))
            def _():
                copy.start()

            shifted.append((same, copy))

        for load in loads:
            load.wait()
        for p in range(parts):
            zz = c * parts + p
            for r in range(cores):
                to = turn(c, r, cores)
                same = jnp.logical_and(zz == z, to == c)
                unless(same, remote(
                    kv_src.at[p, to], kv_all.at[x, z, to], kv_send.at[p, r],
                    kv_recv.at[z], at_core(zz, to),
                ))

                @pl.when(same)
                def _(p=p, to=to):
                    kv_all[x, z, to] = kv_src[p, to]

            same = jnp.logical_and(zz == z, taker == c)
            unless(same, remote(
                q_src.at[p], q_all.at[half], q_send.at[p], q_recv.at[half],
                at_core(zz, taker),
            ))

            @pl.when(same)
            def _(p=p):
                q_all[half] = q_src[p]

        for load in weight_loads:
            load.wait()
        send_column(0, range(1))
        send_column(1, range(1))
        spread_block(0, 0)

        def from_z(dz):
            return turn(z, along - dz, along)

        def keys(bx, dz, core):
            return kv_all.at[turn(x, bx, across), from_z(dz), core]

        def await_keys(held, sem):
            remote(held, held, kv_send.at[0, 0], sem, place(dc=1)).wait_recv()

        def to_twin(bx, dz, dc):
            held = keys(bx, dz, c)
            launch(remote(
                held, held, twin_send.at[bx, dz, dc], twin_recv.at[bx, dz, dc], place(dc=dc)
            ))

        for dz in everywhere:
            if dz:
                await_keys(keys(0, dz, c), kv_recv.at[from_z(dz)])
            else:
                @pl.when(source != c)
                def _():
                    await_keys(keys(0, 0, c), kv_recv.at[z])
            held = keys(0, dz, c)
            for dx in range(1, across):
                launch(remote(
                    held, held, over_send.at[dx, dz],
                    over_recv.at[across - dx, dz], place(dx=dx),
                ))
            for dc in range(1, cores):
                to_twin(0, dz, dc)
        send_column(0, far_first[:1])
        for bx in range(1, across):
            for dz in everywhere:
                await_keys(keys(bx, dz, c), over_recv.at[bx, dz])
                for dc in range(1, cores):
                    to_twin(bx, dz, dc)
        spread_block(1, 0)
        for bx in range(across):
            for dz in everywhere:
                for dc in range(1, cores):
                    await_keys(
                        keys(bx, dz, turn(c, cores - dc, cores)), twin_recv.at[bx, dz, dc]
                    )

        lane = lax.broadcasted_iota(jnp.int32, (tok, wide_part), 1)

        def lanes_of(h, size):
            return jnp.logical_and(lane >= h * size, lane < (h + 1) * size)

        def block_of(bx, bz, diagonal):
            scored = []
            for kind, (_, _, _, _, size) in enumerate(kinds):
                held = kv_all.at[bx, bz, kind]
                lines = held[pl.ds(2 * tok, pad), :].astype(F32) * LOG2E
                for h in range(wide_part // size):
                    first = h * row_parts
                    offset = jnp.concatenate(
                        [lines[first + i : first + i + 1] for i in range(row_parts)], axis=1
                    )
                    scores = lax.dot_general(
                        masked[kind, h], held[pl.ds(0, tok), :], (((1,), (1,)), ((), ())),
                        preferred_element_type=F32,
                    )
                    scored.append((kind, h, scores * (size ** -0.5 * LOG2E) + offset))
            weighed = [(kind, h, *weigh(scores, diagonal)) for kind, h, scores in scored]
            for kind, (_, _, _, _, size) in enumerate(kinds):
                values = kv_all[bx, bz, kind, pl.ds(tok, tok), :]
                own = [(h, w, used) for which, h, w, used in weighed if which == kind]
                added, total = None, None
                for h, w, used in own:
                    kept = values
                    if len(own) > 1:
                        kept = jnp.where(lanes_of(h, size), values, jnp.zeros_like(values))
                    product = jnp.dot(w, kept, preferred_element_type=F32)
                    used = jnp.broadcast_to(used, (tok, wide_part))
                    added = product if added is None else added + product
                    total = used if total is None else jnp.where(lanes_of(h, size), used, total)
                if diagonal:
                    running[kind] = added
                    spent[kind] = total
                else:
                    running[kind] = running[kind] + added * jnp.exp2(-spent[kind])
                    spent[kind] = spent[kind] + total

        def sweep(zq, slot):
            shard = zq * across + x
            for kind, (_, _, _, _, size) in enumerate(kinds):
                queries = q_all[slot, kind]
                for h in range(wide_part // size):
                    masked[kind, h] = jnp.where(
                        lanes_of(h, size), queries, jnp.zeros_like(queries)
                    )
            block_of(x, zq, True)

            def one(t):
                at = shard - 1 - t
                block_of(lax.rem(at, across), lax.div(at, across), False)

            each(0, shard, one)
            same = jnp.logical_and(zq == z, source == c)
            for kind, (q, _, _, _, _) in enumerate(kinds):
                at = kind * q.shape[1] + share * wide_part
                cols = pl.ds(pl.multiple_of(at, wide_part), wide_part)
                back[slot, kind] = running[kind].astype(BF16)
                unless(same, remote(
                    back.at[slot, kind], mixed.at[:, cols], back_send.at[slot, kind],
                    back_recv.at[share, kind], at_core(zq, source),
                ))

                @pl.when(same)
                def _(kind=kind, cols=cols):
                    mixed[:, cols] = running[kind].astype(BF16)

        for slot in range(2):
            zq = c if slot == 0 else along - 1 - c

            @pl.when(jnp.logical_not(jnp.logical_and(zq == z, source == c)))
            def _(slot=slot):
                remote(
                    q_all.at[slot], q_all.at[slot], q_send.at[0], q_recv.at[slot], place(dc=1)
                ).wait_recv()

            sweep(zq, slot)
            relay_block(slot, 0)
        send_column(0, far_first[1:2])
        for dz in far_first[:1]:
            spread_block(0, dz)
        for p in range(parts):
            same = jnp.logical_and(c * parts + p == z, taker == c)

            @pl.when(jnp.logical_not(same))
            def _(p=p):
                for kind, (q, _, _, _, _) in enumerate(kinds):
                    held = mixed.at[:, pl.ds(kind * q.shape[1] + p * wide_part, wide_part)]
                    remote(
                        held, held, back_send.at[0, 0], back_recv.at[p, kind], place(dc=1)
                    ).wait_recv()

        send_column(0, far_first[2:])
        send_column(1, far_first[:1])

        def drain():
            for same, copy in shifted:
                @pl.when(jnp.logical_not(same))
                def _(copy=copy):
                    copy.wait_send()

        return drain

    drain = column_attention() if column else ring_attention()

    chunks = 4
    width = model // chunks

    def chunk(k):
        return pl.ds(k * width, width)

    def twins(k, dc):
        return remote(
            twin_out.at[dc - 1, :, chunk(k)], twin_in.at[dc - 1, :, chunk(k)],
            t_send.at[k, dc - 1], t_recv.at[k, dc - 1], place(dc=dc),
        )

    def others(k, dy):
        return remote(
            lane_out.at[dy - 1, :, chunk(k)], lane_in.at[dy - 1, :, chunk(k)],
            l_send.at[k, dy - 1], l_recv.at[k, dy - 1], place(dy=dy),
        )

    def part_rows(lane, core):
        return pl.ds(pl.multiple_of((lane * cores + core) * rows, rows), rows)

    def paired(lane, k):
        found = part[part_rows(lane, c), chunk(k)]
        at = pl.ds(pl.multiple_of(lane * rows, rows), rows)
        for dc in range(1, cores):
            found = found + twin_in[dc - 1, at, chunk(k)].astype(F32)
        return found

    for k in range(chunks):
        part[:, chunk(k)] = jnp.dot(
            mixed[...], out_all[:, chunk(k)], preferred_element_type=F32
        )
        for dc in range(1, cores):
            for lane in range(lanes):
                twin_out[dc - 1, pl.ds(lane * rows, rows), chunk(k)] = part[
                    part_rows(lane, turn(c, dc, cores)), chunk(k)
                ].astype(BF16)
            launch(twins(k, dc))
    for k in range(chunks):
        for dc in range(1, cores):
            twins(k, dc).wait_recv()
        for dy in range(1, lanes):
            lane_out[dy - 1, :, chunk(k)] = paired(turn(y, dy, lanes), k).astype(BF16)
            launch(others(k, dy))
    if not column:
        relay_block(0, 0)
        relay_block(1, 0)
    for dz in far_first[:1]:
        relay_block(0, dz)
    for dz in far_first[1:2]:
        spread_block(0, dz, y_too=False)
    for k in range(chunks):
        total = residual[:, chunk(k)].astype(F32) + paired(y, k)
        for dy in range(1, lanes):
            others(k, dy).wait_recv()
            total = total + lane_in[dy - 1, :, chunk(k)].astype(F32)
        updated[:, chunk(k)] = total
    value = updated[...]
    scale = lax.rsqrt(jnp.mean(value * value, axis=-1, keepdims=True) + 1e-06)

    def rows_of(zz, cc):
        return pl.ds(pl.multiple_of((zz * cores + cc) * rows, rows), rows)

    normed_all[rows_of(z, c), :] = (value * scale * gain[...]).astype(BF16)

    def rows_at(zz):
        return normed_all.at[rows_of(zz, c)]

    def pass_line(zz, way, step):
        to = z + (-1 if way else 1)
        return remote(
            rows_at(zz), rows_at(zz), n_send.at[way, step], n_recv.at[way, step],
            (to * across + x, me_tp),
        )

    def pass_twin(zz, way, step, dc):
        return remote(
            rows_at(zz), rows_at(zz), w_send.at[way, step, dc], w_recv.at[way, step, dc],
            place(dc=dc),
        )

    chained = []

    def when(wanted, copy):
        @pl.when(wanted)
        def _():
            copy.start()

        chained.append((wanted, copy))

    def can_go(way):
        return z > 0 if way else z < along - 1

    for way in range(2):
        when(can_go(way), pass_line(z, way, 0))
    for dc in range(1, cores):
        launch(pass_twin(z, 0, 0, dc))

    def follow(step):
        for way in range(2):
            zz = z + step if way else z - step
            there = zz < along if way else zz >= 0

            @pl.when(there)
            def _(way=way, zz=zz):
                pass_line(zz, way, step - 1).wait_recv()

            if step < along - 1:
                when(jnp.logical_and(there, can_go(way)), pass_line(zz, way, step))
            for dc in range(1, cores):
                when(there, pass_twin(zz, way, step, dc))

    for dz in far_first[1:2]:
        spread_block(0, dz, x_too=False)
    for dz in far_first[2:]:
        spread_block(0, dz)
    strip = model // along

    def strip_of(dz):
        start = turn(z, along - dz, along) * strip
        return pl.ds(pl.multiple_of(start, strip), strip)

    def group_rows(zz):
        return pl.ds(pl.multiple_of(zz * rows, rows), rows)

    def halves(k, zz, dc):
        return remote(
            half_out.at[dc - 1, group_rows(zz), strip_of(k)],
            half_in.at[dc - 1, group_rows(zz), strip_of(k)],
            h_send.at[k, zz, dc - 1], h_recv.at[k, zz, dc - 1], place(dc=dc),
        )

    def sums(k, dz):
        return remote(
            rows_out.at[dz - 1, :, strip_of(k)], rows_in.at[dz - 1, :, strip_of(k)],
            r_send.at[k, dz - 1], r_recv.at[k, dz - 1], place(dz=dz),
        )

    def gathered(zz, cols):
        found = channel[rows_of(zz, c), cols]
        at = pl.ds(pl.multiple_of(zz * rows, rows), rows)
        for dc in range(1, cores):
            found = found + half_in[dc - 1, at, cols].astype(F32)
        return found

    def share_rows(k, zz):
        for dc in range(1, cores):
            half_out[dc - 1, group_rows(zz), strip_of(k)] = channel[
                rows_of(zz, turn(c, dc, cores)), strip_of(k)
            ].astype(BF16)
            halves(k, zz, dc).start()

    def hand_rows(k, dz):
        zz = turn(z, dz, along)
        for dc in range(1, cores):
            halves(k, zz, dc).wait_recv()
        rows_out[dz - 1, :, strip_of(k)] = gathered(zz, strip_of(k)).astype(BF16)
        sums(k, dz).start()

    def slab(zz):
        return pl.ds(pl.multiple_of(zz * cores * rows, cores * rows), cores * rows)

    def descend_rows(k, zz):
        def one(i):
            shard = origin(k) - x + i
            cols = pl.ds(pl.multiple_of(shard * depth, depth), depth)
            channel[slab(zz), cols] = jnp.dot(
                hidden[slab(zz), :], down_buf[shard], preferred_element_type=F32
            )

        each(0, across, one)
        share_rows(k, zz)

    def climb(zz):
        def one(i):
            product = jnp.dot(
                normed_all[slab(zz), :], up_buf[i], preferred_element_type=F32
            )
            cols = pl.ds(pl.multiple_of(i * unit, unit), unit)
            hidden[slab(zz), cols] = jnp.square(jnp.maximum(product, 0.0)).astype(BF16)

        each(0, peers, one)

    def sides(step, body):
        def side(way):
            zz = jnp.where(way == 1, z + step, z - step)

            @pl.when(jnp.logical_and(zz >= 0, zz < along))
            def _():
                body(way, zz)

        each(0, 2, side)

    early = [0]
    final_step = max(beyond)

    def work(step):
        def body(way, zz):
            for dc in range(1, cores):
                pass_twin(zz, way, step, dc).wait_recv()
            climb(zz)
            for k in early:
                descend_rows(k, zz)

        sides(step, body)

    def hand(step):
        def body(way, zz):
            for k in early:
                hand_rows(k, turn(zz, along - z, along))

        sides(step, body)

    def pass_on(step):
        follow(step)
        send_column(1, far_first[step : step + 1])

    pass_on(1)
    for dz in far_first[1:]:
        relay_block(0, dz)
    for dz in far_first[:1]:
        spread_block(1, dz)
    for step in beyond[1:-1]:
        pass_on(step)
    for dz in far_first[1:2]:
        spread_block(1, dz)
    for dz in far_first[:1]:
        relay_block(1, dz)
    for dz in everywhere:
        finish_block(0, dz)
    for k in early:
        finish_block(1, k)
    for step in beyond[:-1]:
        work(step)
        if step > 1:
            hand(step - 1)
    for step in beyond[:-1][-1:]:
        hand(step)
    if final_step > 1:
        pass_on(final_step)
    for dz in far_first[1:2]:
        relay_block(1, dz)
    for dz in far_first[2:]:
        spread_block(1, dz)
    work(final_step)
    for dc in range(1, cores):
        pass_twin(z, 0, 0, dc).wait_recv()
    climb(z)
    for k in early:
        descend_rows(k, z)
    hand(final_step)

    def descend(k):
        finish_block(1, k)

        def one(i):
            shard = origin(k) - x + i
            cols = pl.ds(pl.multiple_of(shard * depth, depth), depth)
            channel[:, cols] = jnp.dot(
                hidden[...], down_buf[shard], preferred_element_type=F32
            )

        each(0, across, one)
        for zz in everywhere:
            share_rows(k, zz)

    for i, k in enumerate(far_first):
        descend(k)
        if i == len(far_first) - 2:
            relay_block(1, far_first[-1])
        for dz in far_first:
            hand_rows(k, dz)
    for k in everywhere:
        for dc in range(1, cores):
            halves(k, z, dc).wait_recv()
    for k in everywhere:
        for dz in range(1, along):
            sums(k, dz).wait_recv()
    for k in everywhere:
        cols = pl.ds(k * strip, strip)
        total = updated[:, cols] + gathered(z, cols)
        for dz in range(1, along):
            total = total + rows_in[dz - 1, :, cols].astype(F32)
        o_ref[:, cols] = total.astype(BF16)

    drain()
    for k in everywhere:
        for dz in beyond:
            sums(k, dz).wait_send()
        for zz in everywhere:
            for dc in range(1, cores):
                halves(k, zz, dc).wait_send()
    for wanted, copy in chained:
        @pl.when(wanted)
        def _(copy=copy):
            copy.wait_send()

    for copy in started:
        copy.wait_send()


def local(
    shards, peers, order, across, cores,
    query_narrow, key_narrow, value_narrow, query_broad, key_broad, value_broad,
    offset_narrow, offset_broad, residual, out_narrow, out_broad, norm_gain, up_proj, down_proj,
):
    tok, columns = query_narrow.shape
    rows, model = residual.shape
    depth, wide = up_proj.shape
    along, lanes = shards // across, peers // cores
    group = along * cores
    unit = wide // group
    chunks = 4
    pad = 16
    parts = max(1, along // cores)
    part_columns = columns // parts
    column = (
        along == 2 * cores
        and columns % parts == 0
        and part_columns % BROAD_SIZE == 0
        and tok % part_columns == 0
    )

    def padded(offset):
        if column:
            return offset
        return jnp.pad(offset, ((0, pad - offset.shape[0]), (0, 0)))

    vmem = pl.BlockSpec(memory_space=pltpu.VMEM)
    anywhere = pl.BlockSpec(memory_space=pl.ANY)
    dma = pltpu.SemaphoreType.DMA
    if column:
        span = 2 * tok + pad
        in_specs = [anywhere] * 6 + [vmem] * 3 + [anywhere] * 2 + [vmem] + [anywhere] * 2
        attention_scratch = [
            pltpu.VMEM((parts, 2, span, part_columns), BF16),
            pltpu.VMEM((parts, 2, tok, part_columns), BF16),
            pltpu.VMEM((across, along, 2, span, part_columns), BF16),
            pltpu.VMEM((2, 2, tok, part_columns), BF16),
            pltpu.VMEM((2, part_columns // NARROW_SIZE, tok, part_columns), BF16),
            pltpu.VMEM((2, tok, part_columns), F32),
            pltpu.VMEM((2, tok, part_columns), F32),
            pltpu.VMEM((2, 2, tok, part_columns), BF16),
            dma((parts, cores)),
            dma((along,)),
            dma((parts,)),
            dma((2,)),
            dma((across, along)),
            dma((across, along)),
            dma((across, along, cores)),
            dma((across, along, cores)),
            dma((2, 2)),
            dma((parts, 2)),
        ]
    else:
        in_specs = [vmem] * 2 + [anywhere] * 6 + [vmem] + [anywhere] * 2 + [vmem] + [anywhere] * 2
        attention_scratch = [
            pltpu.VMEM((2, shards, 2 * tok, columns), BF16),
            pltpu.VMEM((2, shards, pad, tok), BF16),
            dma((2, 3, shards)),
            dma((2, 3, shards)),
        ]
    return pl.pallas_call(
        functools.partial(kernel, shards, peers, order, across, cores, column),
        out_shape=jax.ShapeDtypeStruct((rows, model), BF16),
        in_specs=in_specs,
        out_specs=vmem,
        scratch_shapes=[
            pltpu.VMEM((group, depth, unit), BF16),
            pltpu.VMEM((wide, depth), BF16),
            pltpu.VMEM((peers, model, unit), BF16),
            pltpu.VMEM((shards, peers * unit, depth), BF16),
            pltpu.VMEM((2 * columns, model), BF16),
            pltpu.VMEM((tok, 2 * columns), BF16),
            pltpu.VMEM((tok, model), F32),
            pltpu.VMEM((cores - 1, lanes * rows, model), BF16),
            pltpu.VMEM((cores - 1, lanes * rows, model), BF16),
            pltpu.VMEM((lanes - 1, rows, model), BF16),
            pltpu.VMEM((lanes - 1, rows, model), BF16),
            pltpu.VMEM((rows, model), F32),
            pltpu.VMEM((group * rows, model), BF16),
            pltpu.VMEM((group * rows, peers * unit), BF16),
            pltpu.VMEM((group * rows, model), F32),
            pltpu.VMEM((cores - 1, along * rows, model), BF16),
            pltpu.VMEM((cores - 1, along * rows, model), BF16),
            pltpu.VMEM((along - 1, rows, model), BF16),
            pltpu.VMEM((along - 1, rows, model), BF16),
            dma((2, along, cores)),
            dma((2, along, cores)),
            dma((2, along, cores, lanes, across)),
            dma((2, along, cores, across, lanes)),
            dma((2, along, cores, across, lanes)),
            dma((chunks, cores)),
            dma((chunks, cores)),
            dma((chunks, lanes)),
            dma((chunks, lanes)),
            dma((2, along)),
            dma((2, along)),
            dma((2, along, cores)),
            dma((2, along, cores)),
            dma((along, along, cores)),
            dma((along, along, cores)),
            dma((along, along)),
            dma((along, along)),
            dma((group + 5,)),
            dma((6 * max(parts, 1),)),
        ] + attention_scratch,
        compiler_params=pltpu.CompilerParams(
            collective_id=0, has_side_effects=True, vmem_limit_bytes=60 << 20
        ),
    )(
        query_narrow, query_broad, key_narrow, value_narrow, key_broad, value_broad,
        padded(offset_narrow), padded(offset_broad), residual, out_narrow, out_broad,
        norm_gain.reshape(1, -1), up_proj, down_proj,
    )


def solution(mesh):
    shards, peers = mesh.shape["sp"], mesh.shape["tp"]
    across = 1 << ((shards.bit_length() - 1) // 2)
    return jax.shard_map(
        functools.partial(local, shards, peers, tuple(ring_order(shards)), across, 2),
        mesh=mesh,
        in_specs=(
            P("sp", "tp"),
            P("sp", "tp"),
            P("sp", "tp"),
            P("sp", "tp"),
            P("sp", "tp"),
            P("sp", "tp"),
            P("tp", "sp"),
            P("tp", "sp"),
            P(("sp", "tp"), None),
            P("tp", None),
            P("tp", None),
            P(),
            P("sp", "tp"),
            P("tp", "sp"),
        ),
        out_specs=P(("sp", "tp"), None),
        check_vma=False,
    )
```

```python
import functools
import math

import jax
import jax.numpy as jnp
from jax import lax
from jax.experimental import pallas as pl
from jax.experimental.pallas import tpu as pltpu
from jax.sharding import PartitionSpec as P

NARROW_SIZE = 64
BROAD_SIZE = 128
F32 = jnp.float32
BF16 = jnp.bfloat16
LOG2E = math.log2(math.e)


def ring_order(shards):
    across = 1 << ((shards.bit_length() - 1) // 2)
    along = shards // across
    order = [z * across for z in range(along)]
    for turn, z in enumerate(reversed(range(along))):
        row = list(range(1, across))
        if turn % 2:
            row.reverse()
        order += [z * across + x for x in row]
    return order


def lookup(table, index):
    found = jnp.int32(0)
    for place, value in enumerate(table):
        found = found + jnp.where(index == place, jnp.int32(value), jnp.int32(0))
    return found


def kernel(
    shards, peers, order, across, cores, column,
    q_n, q_b, k_n, v_n, k_b, v_b, off_n, off_b, residual, out_n, out_b, gain, up, down,
    o_ref,
    up_src, down_src, up_buf, down_buf, out_all, mixed, part, twin_out, twin_in,
    lane_out, lane_in, updated,
    normed_all, hidden, channel, half_out, half_in, rows_out, rows_in,
    a_send, a_recv, x_send, y_send, b_recv, t_send, t_recv, l_send, l_recv,
    n_send, n_recv, w_send, w_recv, h_send, h_recv, r_send, r_recv, load_sems, attention_sems,
    *attention_scratch,
):
    tok = q_n.shape[0]
    model = part.shape[1]
    rows = residual.shape[0]
    depth, wide = up.shape
    along, lanes = shards // across, peers // cores
    group = along * cores
    unit = wide // group
    me = lax.axis_index("sp")
    me_tp = lax.axis_index("tp")
    z, x = lax.div(me, across), lax.rem(me, across)
    y, c = lax.div(me_tp, cores), lax.rem(me_tp, cores)

    def turn(value, by, size):
        return lax.rem(value + by, size)

    def place(dz=0, dx=0, dy=0, dc=0):
        return (
            turn(z, dz, along) * across + turn(x, dx, across),
            turn(y, dy, lanes) * cores + turn(c, dc, cores),
        )

    def remote(src, dst, send_sem, recv_sem, where):
        return pltpu.make_async_remote_copy(
            src_ref=src, dst_ref=dst, send_sem=send_sem, recv_sem=recv_sem,
            device_id=where, device_id_type=pl.DeviceIdType.MESH,
        )

    started = []

    def launch(copy):
        copy.start()
        started.append(copy)

    def piece(m, shard, column):
        if m == 0:
            return up_buf.at[column, pl.ds(pl.multiple_of(shard * depth, depth), depth)]
        return down_buf.at[shard, pl.ds(pl.multiple_of(column * unit, unit), unit)]

    far_first = sorted(range(1, along), key=lambda dz: abs(2 * dz - along))
    columns = out_n.shape[0]
    mine = pl.ds(pl.multiple_of((z * cores + c) * unit, unit), unit)
    weight_loads = [
        (up.at[:, pl.ds(j * unit, unit)], up_src.at[j]) for j in range(group)
    ] + [
        (down, down_src),
        (up.at[:, mine], piece(0, me, me_tp)),
        (down.at[mine], piece(1, me, me_tp)),
        (out_n, out_all.at[pl.ds(0, columns)]),
        (out_b, out_all.at[pl.ds(columns, columns)]),
    ]
    weight_loads = [
        pltpu.make_async_copy(src, dst, load_sems.at[i])
        for i, (src, dst) in enumerate(weight_loads)
    ]

    def begin(loads):
        loads = [
            pltpu.make_async_copy(src, dst, attention_sems.at[i])
            for i, (src, dst) in enumerate(loads)
        ]
        for load in loads + weight_loads:
            load.start()
        return loads

    friends = [
        place(dz=dz, dc=dc) for dz in range(along) for dc in range(cores) if dz or dc
    ]
    friends += [place(dx=dx) for dx in range(1, across)]
    friends += [place(dy=dy, dc=dc) for dy in range(1, lanes) for dc in range(cores)]

    def meet():
        barrier = pltpu.get_barrier_semaphore()
        for friend in friends:
            pl.semaphore_signal(
                barrier, inc=1, device_id=friend, device_id_type=pl.DeviceIdType.MESH
            )
        pl.semaphore_wait(barrier, len(friends))

    def each(first, last, body):
        def step(t, carry):
            body(t)
            return carry

        lax.fori_loop(first, last, step, 0)

    def exchange(m, dz, dc):
        to = turn(z, dz, along) * cores + turn(c, dc, cores)
        if m == 0:
            src = up_src.at[to]
        else:
            src = down_src.at[pl.ds(pl.multiple_of(to * unit, unit), unit)]
        return remote(
            src, piece(m, me, me_tp), a_send.at[m, dz, dc], a_recv.at[m, dz, dc],
            place(dz=dz, dc=dc),
        )

    def send_column(m, hops):
        for dz in hops:
            for dc in range(cores):
                if dz or dc:
                    launch(exchange(m, dz, dc))

    def origin(dz, bx=0):
        return turn(z, along - dz, along) * across + turn(x, bx, across)

    def part_of(m, dz, dc, bx, by):
        core = turn(c, cores - dc, cores)
        return piece(m, origin(dz, bx), turn(y, by, lanes) * cores + core)

    def along_x(m, dz, dc, by, dx):
        held = part_of(m, dz, dc, 0, by)
        return remote(
            held, held, x_send.at[m, dz, dc, by, dx],
            b_recv.at[m, dz, dc, (across - dx) % across, by], place(dx=dx),
        )

    def along_y(m, dz, dc, bx, dy):
        held = part_of(m, dz, dc, bx, 0)
        return remote(
            held, held, y_send.at[m, dz, dc, bx, dy],
            b_recv.at[m, dz, dc, bx, (lanes - dy) % lanes], place(dy=dy),
        )

    def await_part(m, dz, dc, bx, by):
        held = part_of(m, dz, dc, bx, by)
        remote(
            held, held, x_send.at[m, dz, dc, 0, 0], b_recv.at[m, dz, dc, bx, by], place(dc=1)
        ).wait_recv()

    arrived = set()

    def spread_part(m, dz, dc, x_too=True, y_too=True):
        if (m, dz, dc) not in arrived:
            arrived.add((m, dz, dc))
            if dz or dc:
                exchange(m, dz, dc).wait_recv()
        if x_too:
            for dx in range(1, across):
                launch(along_x(m, dz, dc, 0, dx))
        if y_too:
            for dy in range(1, lanes):
                launch(along_y(m, dz, dc, 0, dy))

    def spread_block(m, dz, x_too=True, y_too=True):
        for dc in range(cores):
            spread_part(m, dz, dc, x_too, y_too)

    def x_first(dz, dc):
        return (dz + dc) % 2 == 0

    def relay_block(m, dz):
        for dc in range(cores):
            if x_first(dz, dc):
                for bx in range(1, across):
                    await_part(m, dz, dc, bx, 0)
                    for dy in range(1, lanes):
                        launch(along_y(m, dz, dc, bx, dy))
            else:
                for by in range(1, lanes):
                    await_part(m, dz, dc, 0, by)
                    for dx in range(1, across):
                        launch(along_x(m, dz, dc, by, dx))

    def finish_block(m, dz):
        for dc in range(cores):
            for bx in range(across):
                for by in range(lanes):
                    if bx and by or (by if x_first(dz, dc) else bx):
                        await_part(m, dz, dc, bx, by)

    everywhere = range(along)
    beyond = range(1, along)
    row_at = lax.broadcasted_iota(jnp.int32, (tok, tok), 0)
    col_at = lax.broadcasted_iota(jnp.int32, (tok, tok), 1)
    later = (row_at > col_at).astype(BF16)
    before = col_at < row_at

    def ring_attention():
        kv_slots, off_slots, kv_send, kv_recv = attention_scratch
        inverse = [order.index(s) for s in range(shards)]
        pos = lookup(inverse, me)
        right = lookup(order, lax.rem(pos + 1, shards))
        left = lookup(order, lax.rem(pos + shards - 1, shards))
        loads = []
        for way, (k, v, off) in enumerate(((k_n, v_n, off_n), (k_b, v_b, off_b))):
            loads += [
                (k, kv_slots.at[way, 0, pl.ds(0, tok)]),
                (v, kv_slots.at[way, 0, pl.ds(tok, tok)]),
                (off, off_slots.at[way, 0]),
            ]
        loads = begin(loads)
        meet()

        def stream(kind, way, t):
            if kind == 0:
                return off_slots.at[way, t]
            return kv_slots.at[way, t, pl.ds((kind - 1) * tok, tok)]

        def hop(kind, way, t):
            return remote(
                stream(kind, way, t), stream(kind, way, t + 1),
                kv_send.at[way, kind, t], kv_recv.at[way, kind, t],
                ((left if way else right), me_tp),
            )

        def relay(t):
            for kind in range(3):
                for way in range(2):
                    hop(kind, way, t - 1).wait_recv()
                    hop(kind, way, t).start()

        for load in loads:
            load.wait()
        for kind in range(3):
            for way in range(2):
                hop(kind, way, 0).start()
        for load in weight_loads:
            load.wait()
        each(1, shards - 1, relay)
        for kind in range(3):
            for way in range(2):
                hop(kind, way, shards - 2).wait_recv()
        for m in range(2):
            send_column(m, range(1))
        send_column(0, beyond)
        for m in range(2):
            spread_block(m, 0)

        def head_block(way, h, size, q, at, keep_sum, diagonal):
            there = lookup(inverse, at)
            slot = lax.rem((there - pos if way else pos - there) + shards, shards)
            cols = pl.ds(h * size, size)
            keys = kv_slots[way, slot, pl.ds(0, tok), cols]
            values = kv_slots[way, slot, pl.ds(tok, tok), cols]
            offset = off_slots[way, slot].astype(F32)[h : h + 1, :]
            scores = lax.dot_general(
                q[:, cols], keys, (((1,), (1,)), ((), ())), preferred_element_type=F32
            ) * (size ** -0.5 * LOG2E) + offset * LOG2E
            weight, spent = weigh(scores, diagonal, keep_sum)
            added = jnp.dot(weight, values, preferred_element_type=F32)
            return keep_sum + spent, added

        for way, (q, size) in enumerate(((q_n, NARROW_SIZE), (q_b, BROAD_SIZE))):
            for h in range(q.shape[1] // size):
                start = head_block(way, h, size, q, me, jnp.zeros((tok, 1), F32), True)

                def sweep(at, state, way=way, h=h, size=size, q=q):
                    keep_sum, running = state
                    keep_sum, added = head_block(
                        way, h, size, q, me - 1 - at, keep_sum, False
                    )
                    return keep_sum, running + added

                _, running = lax.fori_loop(0, me, sweep, start)
                mixed[:, pl.ds(way * q.shape[1] + h * size, size)] = running.astype(BF16)
        for dz in far_first[:1]:
            spread_block(0, dz)

        def drain(t):
            for kind in range(3):
                for way in range(2):
                    hop(kind, way, t).wait_send()

        return lambda: each(0, shards - 1, drain)

    def weigh(scores, diagonal, spent_before=None):
        spent = jnp.maximum(
            scores, jnp.log2(1.0 + jnp.exp2(jnp.minimum(scores, 126.0)))
        )
        breaks = scores - spent
        if diagonal:
            spent = jnp.where(before, spent, 0.0)
        rounded = spent.astype(BF16)
        after = jnp.dot(rounded, later, preferred_element_type=F32)
        power = breaks - after
        if spent_before is not None:
            power = power - spent_before
        weight = jnp.exp2(power)
        if diagonal:
            weight = jnp.where(before, weight, 0.0)
        return weight.astype(BF16), after[:, :1] + rounded[:, :1].astype(F32)

    def column_attention():
        (
            kv_src, q_src, kv_all, q_all, masked, running, spent, back,
            kv_send, kv_recv, q_send, q_recv, over_send, over_recv, twin_send, twin_recv,
            back_send, back_recv,
        ) = attention_scratch
        parts = along // cores
        wide_part = q_src.shape[3]
        row_parts = tok // wide_part
        kinds = ((q_n, k_n, v_n, off_n, NARROW_SIZE), (q_b, k_b, v_b, off_b, BROAD_SIZE))
        loads = []
        for p in range(parts):
            cols = pl.ds(p * wide_part, wide_part)
            for kind, (q, k, v, _, _) in enumerate(kinds):
                loads += [
                    (k.at[:, cols], kv_src.at[p, kind, pl.ds(0, tok)]),
                    (v.at[:, cols], kv_src.at[p, kind, pl.ds(tok, tok)]),
                    (q.at[:, cols], q_src.at[p, kind]),
                ]
        loads = begin(loads)
        pad = kv_src.shape[2] - 2 * tok
        for p in range(parts):
            for kind, (_, _, _, off, size) in enumerate(kinds):
                per = wide_part // size
                lines = []
                for h in range(p * per, (p + 1) * per):
                    for i in range(row_parts):
                        lines.append(
                            off[h : h + 1, pl.ds(i * wide_part, wide_part)].astype(F32)
                        )
                lines.append(jnp.zeros((pad - len(lines), wide_part), F32))
                kv_src[p, kind, pl.ds(2 * tok, pad), :] = jnp.concatenate(
                    lines, axis=0
                ).astype(BF16)
        meet()

        source = lax.div(z, parts)
        share = lax.rem(z, parts)
        half = jnp.where(z >= cores, jnp.int32(1), jnp.int32(0))
        taker = jnp.where(z >= cores, along - 1 - z, z)
        shifted = []

        def at_core(zz, core):
            return (zz * across + x, y * cores + core)

        def unless(same, copy):
            @pl.when(jnp.logical_not(same))
            def _():
                copy.start()

            shifted.append((same, copy))

        for load in loads:
            load.wait()
        for p in range(parts):
            zz = c * parts + p
            for r in range(cores):
                to = turn(c, r, cores)
                same = jnp.logical_and(zz == z, to == c)
                unless(same, remote(
                    kv_src.at[p, to], kv_all.at[x, z, to], kv_send.at[p, r],
                    kv_recv.at[z], at_core(zz, to),
                ))

                @pl.when(same)
                def _(p=p, to=to):
                    kv_all[x, z, to] = kv_src[p, to]

            same = jnp.logical_and(zz == z, taker == c)
            unless(same, remote(
                q_src.at[p], q_all.at[half], q_send.at[p], q_recv.at[half],
                at_core(zz, taker),
            ))

            @pl.when(same)
            def _(p=p):
                q_all[half] = q_src[p]

        for load in weight_loads:
            load.wait()
        send_column(0, range(1))
        send_column(1, range(1))
        spread_block(0, 0)

        def from_z(dz):
            return turn(z, along - dz, along)

        def keys(bx, dz, core):
            return kv_all.at[turn(x, bx, across), from_z(dz), core]

        def await_keys(held, sem):
            remote(held, held, kv_send.at[0, 0], sem, place(dc=1)).wait_recv()

        def to_twin(bx, dz, dc):
            held = keys(bx, dz, c)
            launch(remote(
                held, held, twin_send.at[bx, dz, dc], twin_recv.at[bx, dz, dc], place(dc=dc)
            ))

        for dz in everywhere:
            if dz:
                await_keys(keys(0, dz, c), kv_recv.at[from_z(dz)])
            else:
                @pl.when(source != c)
                def _():
                    await_keys(keys(0, 0, c), kv_recv.at[z])
            held = keys(0, dz, c)
            for dx in range(1, across):
                launch(remote(
                    held, held, over_send.at[dx, dz],
                    over_recv.at[across - dx, dz], place(dx=dx),
                ))
            for dc in range(1, cores):
                to_twin(0, dz, dc)
        send_column(0, far_first[:1])
        for bx in range(1, across):
            for dz in everywhere:
                await_keys(keys(bx, dz, c), over_recv.at[bx, dz])
                for dc in range(1, cores):
                    to_twin(bx, dz, dc)
        spread_block(1, 0)
        for bx in range(across):
            for dz in everywhere:
                for dc in range(1, cores):
                    await_keys(
                        keys(bx, dz, turn(c, cores - dc, cores)), twin_recv.at[bx, dz, dc]
                    )

        lane = lax.broadcasted_iota(jnp.int32, (tok, wide_part), 1)

        def lanes_of(h, size):
            return jnp.logical_and(lane >= h * size, lane < (h + 1) * size)

        def block_of(bx, bz, diagonal):
            scored = []
            for kind, (_, _, _, _, size) in enumerate(kinds):
                held = kv_all.at[bx, bz, kind]
                lines = held[pl.ds(2 * tok, pad), :].astype(F32) * LOG2E
                for h in range(wide_part // size):
                    first = h * row_parts
                    offset = jnp.concatenate(
                        [lines[first + i : first + i + 1] for i in range(row_parts)], axis=1
                    )
                    scores = lax.dot_general(
                        masked[kind, h], held[pl.ds(0, tok), :], (((1,), (1,)), ((), ())),
                        preferred_element_type=F32,
                    )
                    scored.append((kind, h, scores * (size ** -0.5 * LOG2E) + offset))
            weighed = [(kind, h, *weigh(scores, diagonal)) for kind, h, scores in scored]
            for kind, (_, _, _, _, size) in enumerate(kinds):
                values = kv_all[bx, bz, kind, pl.ds(tok, tok), :]
                own = [(h, w, used) for which, h, w, used in weighed if which == kind]
                added, total = None, None
                for h, w, used in own:
                    kept = values
                    if len(own) > 1:
                        kept = jnp.where(lanes_of(h, size), values, jnp.zeros_like(values))
                    product = jnp.dot(w, kept, preferred_element_type=F32)
                    used = jnp.broadcast_to(used, (tok, wide_part))
                    added = product if added is None else added + product
                    total = used if total is None else jnp.where(lanes_of(h, size), used, total)
                if diagonal:
                    running[kind] = added
                    spent[kind] = total
                else:
                    running[kind] = running[kind] + added * jnp.exp2(-spent[kind])
                    spent[kind] = spent[kind] + total

        def sweep(zq, slot):
            shard = zq * across + x
            for kind, (_, _, _, _, size) in enumerate(kinds):
                queries = q_all[slot, kind]
                for h in range(wide_part // size):
                    masked[kind, h] = jnp.where(
                        lanes_of(h, size), queries, jnp.zeros_like(queries)
                    )
            block_of(x, zq, True)

            def one(t):
                at = shard - 1 - t
                block_of(lax.rem(at, across), lax.div(at, across), False)

            each(0, shard, one)
            same = jnp.logical_and(zq == z, source == c)
            for kind, (q, _, _, _, _) in enumerate(kinds):
                at = kind * q.shape[1] + share * wide_part
                cols = pl.ds(pl.multiple_of(at, wide_part), wide_part)
                back[slot, kind] = running[kind].astype(BF16)
                unless(same, remote(
                    back.at[slot, kind], mixed.at[:, cols], back_send.at[slot, kind],
                    back_recv.at[share, kind], at_core(zq, source),
                ))

                @pl.when(same)
                def _(kind=kind, cols=cols):
                    mixed[:, cols] = running[kind].astype(BF16)

        for slot in range(2):
            zq = c if slot == 0 else along - 1 - c

            @pl.when(jnp.logical_not(jnp.logical_and(zq == z, source == c)))
            def _(slot=slot):
                remote(
                    q_all.at[slot], q_all.at[slot], q_send.at[0], q_recv.at[slot], place(dc=1)
                ).wait_recv()

            sweep(zq, slot)
            relay_block(slot, 0)
        send_column(0, far_first[1:2])
        for dz in far_first[:1]:
            spread_block(0, dz)
        for p in range(parts):
            same = jnp.logical_and(c * parts + p == z, taker == c)

            @pl.when(jnp.logical_not(same))
            def _(p=p):
                for kind, (q, _, _, _, _) in enumerate(kinds):
                    held = mixed.at[:, pl.ds(kind * q.shape[1] + p * wide_part, wide_part)]
                    remote(
                        held, held, back_send.at[0, 0], back_recv.at[p, kind], place(dc=1)
                    ).wait_recv()

        send_column(0, far_first[2:])
        send_column(1, far_first[:1])

        def drain():
            for same, copy in shifted:
                @pl.when(jnp.logical_not(same))
                def _(copy=copy):
                    copy.wait_send()

        return drain

    drain = column_attention() if column else ring_attention()

    chunks = 4
    width = model // chunks

    def chunk(k):
        return pl.ds(k * width, width)

    def twins(k, dc):
        return remote(
            twin_out.at[dc - 1, :, chunk(k)], twin_in.at[dc - 1, :, chunk(k)],
            t_send.at[k, dc - 1], t_recv.at[k, dc - 1], place(dc=dc),
        )

    def others(k, dy):
        return remote(
            lane_out.at[dy - 1, :, chunk(k)], lane_in.at[dy - 1, :, chunk(k)],
            l_send.at[k, dy - 1], l_recv.at[k, dy - 1], place(dy=dy),
        )

    def part_rows(lane, core):
        return pl.ds(pl.multiple_of((lane * cores + core) * rows, rows), rows)

    def paired(lane, k):
        found = part[part_rows(lane, c), chunk(k)]
        at = pl.ds(pl.multiple_of(lane * rows, rows), rows)
        for dc in range(1, cores):
            found = found + twin_in[dc - 1, at, chunk(k)].astype(F32)
        return found

    for k in range(chunks):
        part[:, chunk(k)] = jnp.dot(
            mixed[...], out_all[:, chunk(k)], preferred_element_type=F32
        )
        for dc in range(1, cores):
            for lane in range(lanes):
                twin_out[dc - 1, pl.ds(lane * rows, rows), chunk(k)] = part[
                    part_rows(lane, turn(c, dc, cores)), chunk(k)
                ].astype(BF16)
            launch(twins(k, dc))
    for k in range(chunks):
        for dc in range(1, cores):
            twins(k, dc).wait_recv()
        for dy in range(1, lanes):
            lane_out[dy - 1, :, chunk(k)] = paired(turn(y, dy, lanes), k).astype(BF16)
            launch(others(k, dy))
    if not column:
        relay_block(0, 0)
        relay_block(1, 0)
    for dz in far_first[:1]:
        relay_block(0, dz)
    for dz in far_first[1:2]:
        spread_block(0, dz, y_too=False)
    for k in range(chunks):
        total = residual[:, chunk(k)].astype(F32) + paired(y, k)
        for dy in range(1, lanes):
            others(k, dy).wait_recv()
            total = total + lane_in[dy - 1, :, chunk(k)].astype(F32)
        updated[:, chunk(k)] = total
    value = updated[...]
    scale = lax.rsqrt(jnp.mean(value * value, axis=-1, keepdims=True) + 1e-06)

    def rows_of(zz, cc):
        return pl.ds(pl.multiple_of((zz * cores + cc) * rows, rows), rows)

    normed_all[rows_of(z, c), :] = (value * scale * gain[...]).astype(BF16)

    def rows_at(zz):
        return normed_all.at[rows_of(zz, c)]

    def pass_line(zz, way, step):
        to = z + (-1 if way else 1)
        return remote(
            rows_at(zz), rows_at(zz), n_send.at[way, step], n_recv.at[way, step],
            (to * across + x, me_tp),
        )

    def pass_twin(zz, way, step, dc):
        return remote(
            rows_at(zz), rows_at(zz), w_send.at[way, step, dc], w_recv.at[way, step, dc],
            place(dc=dc),
        )

    chained = []

    def when(wanted, copy):
        @pl.when(wanted)
        def _():
            copy.start()

        chained.append((wanted, copy))

    def can_go(way):
        return z > 0 if way else z < along - 1

    for way in range(2):
        when(can_go(way), pass_line(z, way, 0))
    for dc in range(1, cores):
        launch(pass_twin(z, 0, 0, dc))

    def follow(step):
        for way in range(2):
            zz = z + step if way else z - step
            there = zz < along if way else zz >= 0

            @pl.when(there)
            def _(way=way, zz=zz):
                pass_line(zz, way, step - 1).wait_recv()

            if step < along - 1:
                when(jnp.logical_and(there, can_go(way)), pass_line(zz, way, step))
            for dc in range(1, cores):
                when(there, pass_twin(zz, way, step, dc))

    for dz in far_first[1:2]:
        spread_block(0, dz, x_too=False)
    for dz in far_first[2:]:
        spread_block(0, dz)
    strip = model // along

    def strip_of(dz):
        start = turn(z, along - dz, along) * strip
        return pl.ds(pl.multiple_of(start, strip), strip)

    def group_rows(zz):
        return pl.ds(pl.multiple_of(zz * rows, rows), rows)

    def halves(k, zz, dc):
        return remote(
            half_out.at[dc - 1, group_rows(zz), strip_of(k)],
            half_in.at[dc - 1, group_rows(zz), strip_of(k)],
            h_send.at[k, zz, dc - 1], h_recv.at[k, zz, dc - 1], place(dc=dc),
        )

    def sums(k, dz):
        return remote(
            rows_out.at[dz - 1, :, strip_of(k)], rows_in.at[dz - 1, :, strip_of(k)],
            r_send.at[k, dz - 1], r_recv.at[k, dz - 1], place(dz=dz),
        )

    def gathered(zz, cols):
        found = channel[rows_of(zz, c), cols]
        at = pl.ds(pl.multiple_of(zz * rows, rows), rows)
        for dc in range(1, cores):
            found = found + half_in[dc - 1, at, cols].astype(F32)
        return found

    def share_rows(k, zz):
        for dc in range(1, cores):
            half_out[dc - 1, group_rows(zz), strip_of(k)] = channel[
                rows_of(zz, turn(c, dc, cores)), strip_of(k)
            ].astype(BF16)
            halves(k, zz, dc).start()

    def hand_rows(k, dz):
        zz = turn(z, dz, along)
        for dc in range(1, cores):
            halves(k, zz, dc).wait_recv()
        rows_out[dz - 1, :, strip_of(k)] = gathered(zz, strip_of(k)).astype(BF16)
        sums(k, dz).start()

    def slab(zz):
        return pl.ds(pl.multiple_of(zz * cores * rows, cores * rows), cores * rows)

    def descend_rows(k, zz):
        def one(i):
            shard = origin(k) - x + i
            cols = pl.ds(pl.multiple_of(shard * depth, depth), depth)
            channel[slab(zz), cols] = jnp.dot(
                hidden[slab(zz), :], down_buf[shard], preferred_element_type=F32
            )

        each(0, across, one)
        share_rows(k, zz)

    def climb(zz):
        def one(i):
            product = jnp.dot(
                normed_all[slab(zz), :], up_buf[i], preferred_element_type=F32
            )
            cols = pl.ds(pl.multiple_of(i * unit, unit), unit)
            hidden[slab(zz), cols] = jnp.square(jnp.maximum(product, 0.0)).astype(BF16)

        each(0, peers, one)

    def sides(step, body):
        def side(way):
            zz = jnp.where(way == 1, z + step, z - step)

            @pl.when(jnp.logical_and(zz >= 0, zz < along))
            def _():
                body(way, zz)

        each(0, 2, side)

    early = [0]
    final_step = max(beyond)

    def work(step):
        def body(way, zz):
            for dc in range(1, cores):
                pass_twin(zz, way, step, dc).wait_recv()
            climb(zz)
            for k in early:
                descend_rows(k, zz)

        sides(step, body)

    def hand(step):
        def body(way, zz):
            for k in early:
                hand_rows(k, turn(zz, along - z, along))

        sides(step, body)

    def pass_on(step):
        follow(step)
        send_column(1, far_first[step : step + 1])

    pass_on(1)
    for dz in far_first[1:]:
        relay_block(0, dz)
    for dz in far_first[:1]:
        spread_block(1, dz)
    for step in beyond[1:-1]:
        pass_on(step)
    for dz in far_first[1:2]:
        spread_block(1, dz)
    for dz in far_first[:1]:
        relay_block(1, dz)
    for dz in everywhere:
        finish_block(0, dz)
    for k in early:
        finish_block(1, k)
    for step in beyond[:-1]:
        work(step)
        if step > 1:
            hand(step - 1)
    for step in beyond[:-1][-1:]:
        hand(step)
    if final_step > 1:
        pass_on(final_step)
    for dz in far_first[1:2]:
        relay_block(1, dz)
    for dz in far_first[2:]:
        spread_block(1, dz)
    work(final_step)
    for dc in range(1, cores):
        pass_twin(z, 0, 0, dc).wait_recv()
    climb(z)
    for k in early:
        descend_rows(k, z)
    hand(final_step)

    def descend(k):
        finish_block(1, k)

        def one(i):
            shard = origin(k) - x + i
            cols = pl.ds(pl.multiple_of(shard * depth, depth), depth)
            channel[:, cols] = jnp.dot(
                hidden[...], down_buf[shard], preferred_element_type=F32
            )

        each(0, across, one)
        for zz in everywhere:
            share_rows(k, zz)

    for i, k in enumerate(far_first):
        descend(k)
        if i == len(far_first) - 2:
            relay_block(1, far_first[-1])
        for dz in far_first[1:] + far_first[:1]:
            hand_rows(k, dz)
    for k in everywhere:
        for dc in range(1, cores):
            halves(k, z, dc).wait_recv()
    for k in everywhere:
        for dz in range(1, along):
            sums(k, dz).wait_recv()
    for k in everywhere:
        cols = pl.ds(k * strip, strip)
        total = updated[:, cols] + gathered(z, cols)
        for dz in range(1, along):
            total = total + rows_in[dz - 1, :, cols].astype(F32)
        o_ref[:, cols] = total.astype(BF16)

    drain()
    for k in everywhere:
        for dz in beyond:
            sums(k, dz).wait_send()
        for zz in everywhere:
            for dc in range(1, cores):
                halves(k, zz, dc).wait_send()
    for wanted, copy in chained:
        @pl.when(wanted)
        def _(copy=copy):
            copy.wait_send()

    for copy in started:
        copy.wait_send()


def local(
    shards, peers, order, across, cores,
    query_narrow, key_narrow, value_narrow, query_broad, key_broad, value_broad,
    offset_narrow, offset_broad, residual, out_narrow, out_broad, norm_gain, up_proj, down_proj,
):
    tok, columns = query_narrow.shape
    rows, model = residual.shape
    depth, wide = up_proj.shape
    along, lanes = shards // across, peers // cores
    group = along * cores
    unit = wide // group
    chunks = 4
    pad = 16
    parts = max(1, along // cores)
    part_columns = columns // parts
    column = (
        along == 2 * cores
        and columns % parts == 0
        and part_columns % BROAD_SIZE == 0
        and tok % part_columns == 0
    )

    def padded(offset):
        if column:
            return offset
        return jnp.pad(offset, ((0, pad - offset.shape[0]), (0, 0)))

    vmem = pl.BlockSpec(memory_space=pltpu.VMEM)
    anywhere = pl.BlockSpec(memory_space=pl.ANY)
    dma = pltpu.SemaphoreType.DMA
    if column:
        span = 2 * tok + pad
        in_specs = [anywhere] * 6 + [vmem] * 3 + [anywhere] * 2 + [vmem] + [anywhere] * 2
        attention_scratch = [
            pltpu.VMEM((parts, 2, span, part_columns), BF16),
            pltpu.VMEM((parts, 2, tok, part_columns), BF16),
            pltpu.VMEM((across, along, 2, span, part_columns), BF16),
            pltpu.VMEM((2, 2, tok, part_columns), BF16),
            pltpu.VMEM((2, part_columns // NARROW_SIZE, tok, part_columns), BF16),
            pltpu.VMEM((2, tok, part_columns), F32),
            pltpu.VMEM((2, tok, part_columns), F32),
            pltpu.VMEM((2, 2, tok, part_columns), BF16),
            dma((parts, cores)),
            dma((along,)),
            dma((parts,)),
            dma((2,)),
            dma((across, along)),
            dma((across, along)),
            dma((across, along, cores)),
            dma((across, along, cores)),
            dma((2, 2)),
            dma((parts, 2)),
        ]
    else:
        in_specs = [vmem] * 2 + [anywhere] * 6 + [vmem] + [anywhere] * 2 + [vmem] + [anywhere] * 2
        attention_scratch = [
            pltpu.VMEM((2, shards, 2 * tok, columns), BF16),
            pltpu.VMEM((2, shards, pad, tok), BF16),
            dma((2, 3, shards)),
            dma((2, 3, shards)),
        ]
    return pl.pallas_call(
        functools.partial(kernel, shards, peers, order, across, cores, column),
        out_shape=jax.ShapeDtypeStruct((rows, model), BF16),
        in_specs=in_specs,
        out_specs=vmem,
        scratch_shapes=[
            pltpu.VMEM((group, depth, unit), BF16),
            pltpu.VMEM((wide, depth), BF16),
            pltpu.VMEM((peers, model, unit), BF16),
            pltpu.VMEM((shards, peers * unit, depth), BF16),
            pltpu.VMEM((2 * columns, model), BF16),
            pltpu.VMEM((tok, 2 * columns), BF16),
            pltpu.VMEM((tok, model), F32),
            pltpu.VMEM((cores - 1, lanes * rows, model), BF16),
            pltpu.VMEM((cores - 1, lanes * rows, model), BF16),
            pltpu.VMEM((lanes - 1, rows, model), BF16),
            pltpu.VMEM((lanes - 1, rows, model), BF16),
            pltpu.VMEM((rows, model), F32),
            pltpu.VMEM((group * rows, model), BF16),
            pltpu.VMEM((group * rows, peers * unit), BF16),
            pltpu.VMEM((group * rows, model), F32),
            pltpu.VMEM((cores - 1, along * rows, model), BF16),
            pltpu.VMEM((cores - 1, along * rows, model), BF16),
            pltpu.VMEM((along - 1, rows, model), BF16),
            pltpu.VMEM((along - 1, rows, model), BF16),
            dma((2, along, cores)),
            dma((2, along, cores)),
            dma((2, along, cores, lanes, across)),
            dma((2, along, cores, across, lanes)),
            dma((2, along, cores, across, lanes)),
            dma((chunks, cores)),
            dma((chunks, cores)),
            dma((chunks, lanes)),
            dma((chunks, lanes)),
            dma((2, along)),
            dma((2, along)),
            dma((2, along, cores)),
            dma((2, along, cores)),
            dma((along, along, cores)),
            dma((along, along, cores)),
            dma((along, along)),
            dma((along, along)),
            dma((group + 5,)),
            dma((6 * max(parts, 1),)),
        ] + attention_scratch,
        compiler_params=pltpu.CompilerParams(
            collective_id=0, has_side_effects=True, vmem_limit_bytes=60 << 20
        ),
    )(
        query_narrow, query_broad, key_narrow, value_narrow, key_broad, value_broad,
        padded(offset_narrow), padded(offset_broad), residual, out_narrow, out_broad,
        norm_gain.reshape(1, -1), up_proj, down_proj,
    )


def solution(mesh):
    shards, peers = mesh.shape["sp"], mesh.shape["tp"]
    across = 1 << ((shards.bit_length() - 1) // 2)
    return jax.shard_map(
        functools.partial(local, shards, peers, tuple(ring_order(shards)), across, 2),
        mesh=mesh,
        in_specs=(
            P("sp", "tp"),
            P("sp", "tp"),
            P("sp", "tp"),
            P("sp", "tp"),
            P("sp", "tp"),
            P("sp", "tp"),
            P("tp", "sp"),
            P("tp", "sp"),
            P(("sp", "tp"), None),
            P("tp", None),
            P("tp", None),
            P(),
            P("sp", "tp"),
            P("tp", "sp"),
        ),
        out_specs=P(("sp", "tp"), None),
        check_vma=False,
    )
```
